512 devices in a mesh: sp: 64 (over z, y), tp: 8 (over x, core).
Axes of the slice: x: 4, y: 8, z: 8, core: 2. Of those that a mesh axis runs over, the one named last changes fastest.
Arguments:
- resid: bfloat16 [32768, 2048], P('sp'), may hold values from -6 to 6
- queries: bfloat16 [32768, 2048], P('sp', 'tp'), may hold values from -6 to 6
- keys: bfloat16 [32768, 512], P('sp', 'tp'), may hold values from -6 to 6
- values: bfloat16 [32768, 512], P('sp', 'tp'), may hold values from -6 to 6
- documents: int32 [32768], P('sp'), may hold values from 0 to 31, never falling along the last dimension, each value on 1 to 2048 neighbouring positions
- q_gain: float32 [64], replicated, may hold values from 0.5 to 6.5
- k_gain: float32 [64], replicated, may hold values from 0.5 to 6.5
- sink: float32 [32], P('tp'), may hold values from -1 to 5
- w_out: bfloat16 [2048, 2048], P('tp'), may hold values from -0.5 to 0.5
- n_gain: float32 [2048], replicated, may hold values from 0.1 to 1.9
- w_up: bfloat16 [2048, 8192], P('sp', 'tp'), may hold values from -0.125 to 0.125
- w_down: bfloat16 [8192, 2048], P('tp', 'sp'), may hold values from -0.0625 to 0.0625
Outputs:
- layer_out: bfloat16 [32768, 2048], P('sp')
The draws below stay inside these ranges and needn't reach their ends.
All inputs are finite; a program needn't handle non-finite values.
Results may differ from the reference program's by a relative error of at most 0.018.
The reference program's roundings to bfloat16 on the way count: a program that leaves them out, or rounds other values in their place, can miss the bound.
Values may be sent and summed in bfloat16 or wider, within the bound.
A program may use at most 64 MiB of HBM per device.

```python
import math
import jax
import jax.numpy as jnp
import numpy as np
from jax import lax

D = 2048
HEADS = 32
KV_HEADS = 8
HEAD = 64
FF = 8192
WINDOW = 128
TOK_DEV = 512
TOKENS = 32768
N_SP = 64
N_TP = 8


def base_keys(key):
    return jax.random.normal(jax.random.fold_in(key, 3), (TOKENS, KV_HEADS * HEAD), jnp.float32)


def draw_keys(key, part):
    drawn = base_keys(key)
    return jnp.clip(drawn, -6.0, 6.0).astype(jnp.bfloat16)


def draw_queries(key, part):
    drawn = jax.random.normal(jax.random.fold_in(key, 7), (TOKENS, HEADS * HEAD), jnp.float32)
    return jnp.clip(drawn, -6.0, 6.0).astype(jnp.bfloat16)


def draw_q_gain(key, part):
    return jax.random.uniform(jax.random.fold_in(key, 21), (HEAD,), jnp.float32, 0.5, 1.5)


def draw_k_gain(key, part):
    return jax.random.uniform(jax.random.fold_in(key, 23), (HEAD,), jnp.float32, 0.5, 1.5)


def block_levels(key, shape, cuts, least, top_value):
    level, own = 1.0, jax.random.fold_in(key, 6)
    for position, shards_of in cuts:
        draws = jnp.exp(jax.random.uniform(jax.random.fold_in(own, position), (shards_of,), jnp.float32, least / len(cuts), top_value / len(cuts)))
        level = level * jnp.repeat(draws, shape[position] // shards_of).reshape([-1 if axis == position else 1 for axis in range(len(shape))])
    return level


def profile(number_of, total, bound, lean):
    loads = [(1 << 20) // math.isqrt(rank ** lean) + 1 for rank in range(2, number_of + 1)]
    rest, holding = total - bound - (number_of - 1), [1] * (number_of - 1)
    while rest > 0:
        candidates = [i for i in range(number_of - 1) if holding[i] < bound]
        mass, budget = sum([loads[i] for i in candidates]), rest
        for i in candidates:
            extra = min(bound - holding[i], max(1, budget * loads[i] // mass), rest)
            holding[i] = holding[i] + extra
            rest = rest - extra
    return np.array([bound] + holding)


def uneven(key, amount, total, limit, lean):
    if amount == 2:
        one = jax.random.randint(key, (), max(1, total - limit), min(limit, total - 1) + 1)
        return jnp.stack([one, total - one])
    sizes = jnp.asarray(profile(amount, total, limit, lean), jnp.int32)
    twos = (amount - 1) // 2
    source_of, taker = sizes[1:1 + 2 * twos:2], sizes[2:2 + 2 * twos:2]
    slack = jnp.minimum(source_of - 1, limit - taker)
    passed = jax.random.randint(jax.random.fold_in(key, 1), (twos,), 0, 1 << 20) % (slack + 1)
    sizes = sizes.at[1:1 + 2 * twos:2].set(source_of - passed).at[2:2 + 2 * twos:2].set(taker + passed)
    return sizes[jax.random.permutation(jax.random.fold_in(key, 2), amount)]


def gaussian(stream_key, extent, deviation, bound, cuts=(), kind=jnp.bfloat16):
    result = jax.random.normal(stream_key, extent, jnp.float32) * deviation
    if len(cuts) > 0:
        result = block_levels(stream_key, extent, cuts, -0.22, 0.18) * result
    return jnp.clip(result, min=-bound, max=bound).astype(kind)


def setup_inputs(seed: int = 0) -> dict:
    splits = jax.random.split(jax.random.key(seed), 13)
    resid = gaussian(splits[0], (TOKENS, D), 1.0, 6.0, ((0, 64),))
    queries = draw_queries(jax.random.fold_in(splits[12], 71), 0)
    keys = draw_keys(jax.random.fold_in(splits[12], 71), 0)
    values = gaussian(splits[3], (TOKENS, KV_HEADS * HEAD), 1.0, 6.0, ((0, 64), (1, 8)))
    documents = jnp.searchsorted(jnp.cumsum(uneven(splits[4], N_SP // 2, TOKENS, 4 * TOK_DEV, 0)), jnp.arange(TOKENS), side="right").astype(jnp.int32)
    q_gain = draw_q_gain(jax.random.fold_in(splits[12], 71), 0)
    k_gain = draw_k_gain(jax.random.fold_in(splits[12], 71), 0)
    sink = jnp.clip(-1.0 + 6.0 * jax.random.uniform(splits[7], (HEADS,), jnp.float32) ** block_levels(splits[7], (HEADS,), ((0, 8),), -0.2, 0.2), -1.0, 5.0)
    w_out = gaussian(splits[8], (HEADS * HEAD, D), (HEADS * HEAD // 16) ** -0.5, 0.5, ((0, 8),))
    n_gain = jnp.clip(1.0 + 0.18 * jax.random.normal(splits[9], (D,), jnp.float32), 0.1, 1.9)
    w_up = gaussian(splits[10], (D, FF), D ** -0.5, 0.125, ((0, 64), (1, 8)))
    w_down = gaussian(splits[11], (FF, D), FF ** -0.5, 0.0625, ((0, 8), (1, 64)))
    return dict(resid=resid, queries=queries, keys=keys, values=values, documents=documents, q_gain=q_gain, k_gain=k_gain, sink=sink, w_out=w_out, n_gain=n_gain, w_up=w_up, w_down=w_down)


EPS = 1e-06

def rms_scale(field, gain):
    wide = field.astype(jnp.float32)
    return wide * lax.rsqrt(lax.optimization_barrier(jnp.mean(wide * wide, axis=-1, keepdims=True)) + EPS) * gain.astype(jnp.float32)

def reference(resid, queries, keys, values, documents, q_gain, k_gain, sink, w_out, n_gain, w_up, w_down):
    group = HEADS // KV_HEADS
    qnorm = rms_scale(queries.reshape(TOKENS, KV_HEADS, group, HEAD), q_gain).astype(jnp.bfloat16)
    knorm = rms_scale(keys.reshape(TOKENS, KV_HEADS, HEAD), k_gain).astype(jnp.bfloat16)
    vheads = values.reshape(TOKENS, KV_HEADS, HEAD)
    padding = ((WINDOW, WINDOW), (0, 0), (0, 0))
    key_pad = jnp.pad(knorm, padding)
    value_pad = jnp.pad(vheads, padding)
    doc_pad = jnp.pad(documents, (WINDOW, WINDOW), constant_values=-1)
    slopes = jnp.exp2(-8.0 * (jnp.arange(HEADS, dtype=jnp.float32) + 1.0) / HEADS).reshape(KV_HEADS, group)
    sink_f = sink.astype(jnp.float32).reshape(KV_HEADS, group)
    span = TOK_DEV
    blocks = TOKENS // span
    query_blocks = qnorm.reshape(blocks, span, KV_HEADS, group, HEAD)
    doc_blocks = documents.reshape(blocks, span)

    def one_block(args):
        qblock, dblock, number = args
        start = number * span
        kblock = lax.dynamic_slice_in_dim(key_pad, start, span + 2 * WINDOW, 0)
        vblock = lax.dynamic_slice_in_dim(value_pad, start, span + 2 * WINDOW, 0)
        dkeys = lax.dynamic_slice_in_dim(doc_pad, start, span + 2 * WINDOW, 0)
        query_pos = start + jnp.arange(span, dtype=jnp.int32)
        key_pos = start - WINDOW + jnp.arange(span + 2 * WINDOW, dtype=jnp.int32)
        distance = key_pos[None, :] - query_pos[:, None]
        allowed = (jnp.abs(distance) <= WINDOW) & (key_pos[None, :] >= 0) & (key_pos[None, :] < TOKENS)
        allowed = allowed & (dkeys[None, :] == dblock[:, None])
        scores = jnp.einsum('rkgd,skd->kgrs', qblock.astype(jnp.float32), kblock.astype(jnp.float32)) * HEAD ** (-0.5)
        scores = scores - slopes[:, :, None, None] * jnp.abs(distance).astype(jnp.float32)[None, None]
        scores = jnp.where(allowed[None, None], scores, jnp.float32(-1e+30))
        highest = jnp.maximum(lax.optimization_barrier(jnp.max(scores, axis=-1)), sink_f[:, :, None])
        weights = jnp.exp(scores - highest[..., None])
        denom = lax.optimization_barrier(jnp.sum(weights, axis=-1)) + jnp.exp(sink_f[:, :, None] - highest)
        rounded = weights.astype(jnp.bfloat16)
        summed = jnp.einsum('kgrs,skd->rkgd', rounded.astype(jnp.float32), vblock.astype(jnp.float32))
        return (summed / denom.transpose(2, 0, 1)[..., None]).astype(jnp.bfloat16)
    attended = lax.map(one_block, (query_blocks, doc_blocks, jnp.arange(blocks, dtype=jnp.int32)))
    attended = attended.reshape(TOKENS, HEADS * HEAD)
    cols = HEADS * HEAD // N_TP
    head_mix = jnp.zeros((TOKENS, D), jnp.float32)
    for index in range(N_TP):
        partial_sum = jnp.dot(attended[:, index * cols:(index + 1) * cols], w_out[index * cols:(index + 1) * cols], preferred_element_type=jnp.float32)
        head_mix = head_mix + partial_sum.astype(jnp.bfloat16).astype(jnp.float32)
    middle = (resid.astype(jnp.float32) + head_mix).astype(jnp.bfloat16)
    normed = rms_scale(middle, n_gain).astype(jnp.bfloat16)
    units = FF // N_TP
    unit_mix = jnp.zeros((TOKENS, D), jnp.float32)
    for index in range(N_TP):
        upward = jnp.dot(normed, w_up[:, index * units:(index + 1) * units], preferred_element_type=jnp.float32)
        active = jnp.square(jax.nn.relu(upward)).astype(jnp.bfloat16)
        partial_sum = jnp.dot(active, w_down[index * units:(index + 1) * units], preferred_element_type=jnp.float32)
        unit_mix = unit_mix + partial_sum.astype(jnp.bfloat16).astype(jnp.float32)
    return (middle.astype(jnp.float32) + unit_mix).astype(jnp.bfloat16)
```

```python
import functools

import jax
import jax.numpy as jnp
from jax import lax
from jax.experimental import pallas as pl
from jax.experimental.pallas import tpu as pltpu
from jax.sharding import PartitionSpec as P

WINDOW = 128
EPS = 1e-06
Z, Y, X, C = 8, 8, 4, 2
MESH = pl.DeviceIdType.MESH
BF, F32 = jnp.bfloat16, jnp.float32
NC1, NC2 = 2, 4


def extended(x, sides, width):
    for axis, dim in sides:
        count, length = (lax.axis_size(axis), x.shape[dim])
        up = [(i, (i + 1) % count) for i in range(count - 1)]
        down = [(j, i) for i, j in up]
        last = lax.slice_in_dim(x, length - width, length, axis=dim)
        initial = lax.slice_in_dim(x, 0, width, axis=dim)
        before = lax.ppermute(last, axis, up)
        after = lax.ppermute(initial, axis, down)
        x = jnp.concatenate([before, x, after], axis=dim)
    return x


def rms_scale(field, gain):
    wide = field.astype(F32)
    return wide * lax.rsqrt(jnp.mean(wide * wide, axis=-1, keepdims=True) + EPS) * gain


def fused(
    att, wout_h, resid_h, gain, wup_h, wdt_h, out,
    WU, WD, WO, RES, PB1, RB1, SND1, RCV1, PB2, RB2, SND2, RCV2, NALL, MID, ACC, ACT,
    loc, g1s, g1r, g2s, g2r, d1s, d1r, n1s, n1r, d2s, d2r, n2s, n2r, a1s, a1r, a2s, a2r,
):
    sp, tp = lax.axis_index("sp"), lax.axis_index("tp")
    z, y = sp // Y, sp % Y
    x, c = tp // C, tp % C
    co = 1 - c

    def at_z(s):
        return (((z + s + Z) % Z) * Y + y, tp)

    def at_y(s):
        return (z * Y + (y + s + Y) % Y, tp)

    def xm(s):
        return (x + s + X) % X

    def at_x(s):
        return (sp, xm(s) * C + c)

    partner = (sp, x * C + co)
    pending = []

    def rc(src, dst, ss, rs, dev):
        return pltpu.make_async_remote_copy(
            src_ref=src, dst_ref=dst, send_sem=ss, recv_sem=rs, device_id=dev, device_id_type=MESH
        )

    def put(src, dst, ss, rs, dev):
        rc(src, dst, ss, rs, dev).start()
        pending.append(lambda: rc(src, dst, ss, rs, dev).wait_send())

    def got(ref, ss, rs):
        rc(ref, ref, ss, rs, partner).wait_recv()

    loads = [
        pltpu.make_async_copy(wup_h, WU.at[y, z], loc.at[0]),
        pltpu.make_async_copy(wdt_h, WD.at[z, y], loc.at[1]),
        pltpu.make_async_copy(wout_h, WO, loc.at[2]),
        pltpu.make_async_copy(
            resid_h.at[pl.ds(pl.multiple_of(tp * 64, 64), 64)], RES, loc.at[3]
        ),
    ]
    for copy in loads:
        copy.start()
    barrier = pltpu.get_barrier_semaphore()
    near = [at_z(1), at_z(-1), at_y(1), at_y(-1), at_x(1), at_x(-1), partner]
    for dev in near:
        pl.semaphore_signal(barrier, inc=1, device_id=dev, device_id_type=MESH)
    loads[0].wait()
    loads[1].wait()
    pl.semaphore_wait(barrier, len(near))

    streams = []
    for w, (buf, ma, mi, dma, dmi) in enumerate(
        ((WU, y, z, at_y, at_z), (WD, z, y, at_z, at_y))
    ):
        for e, s in enumerate((1, -1)):
            streams.append((2 * w + e, buf, ma, mi, dma(s), dmi(s), s, e))

    def minor_off(j):
        return jnp.where(j % 2 == 1, -((j + 1) // 2), j // 2)

    def first_ref(st, d, at_me):
        i, buf, ma, mi, _, _, s, e = st
        dist = d if at_me else d - 1
        ref = buf.at[ma, (mi - s * dist + 8) % 8]
        return ref.at[pl.ds(16 * e, 16)] if d == 4 else ref

    def first_send(st, d):
        i, buf, ma, mi, _, dev, s, e = st
        src = first_ref(st, d, False)
        put(src, src, g1s.at[i, d - 1], g1r.at[i, d - 1], dev)

    def first_got(st, d):
        i = st[0]
        got(first_ref(st, d, True), g1s.at[i, d - 1], g1r.at[i, d - 1])

    def second_copy(st, d, j, m):
        i, buf, ma, mi, dev, _, s, e = st
        src = buf.at[(ma - s * (d - 1) + 8) % 8, (mi + minor_off(j) + 8) % 8]
        return rc(src, src, g2s.at[i, m], g2r.at[i, m], dev)

    def second_got(st, d, j, m):
        i, buf, ma, mi, dev, _, s, e = st
        ref = buf.at[(ma - s * d + 16) % 8, (mi + minor_off(j) + 8) % 8]
        got(ref, g2s.at[i, m], g2r.at[i, m])

    def second_first(j):
        for st in streams:
            second_copy(st, 1, j, j).start()

    def pump(lo, hi):
        def both(m, _):
            d, j = m // 8 + 1, m % 8
            for st in streams:
                second_got(st, d, j, m)
                second_copy(st, d + 1, j, m + 8).start()
            return 0

        def half(m, _, es):
            d, j = m // 8 + 1, m % 8
            for st in streams:
                second_got(st, d, j, m)
                if st[7] in es:
                    second_copy(st, 4, j, m + 8 - 4 * st[7]).start()
            return 0

        def last(m, _):
            for st in streams:
                second_got(st, 4, m - 24 + 4 * st[7], m)
            return 0

        for a, b, f in (
            (0, 16, both),
            (16, 20, functools.partial(half, es=(0,))),
            (20, 24, functools.partial(half, es=(1,))),
            (24, 28, last),
        ):
            a, b = max(a, lo), min(b, hi)
            if a < b:
                lax.fori_loop(a, b, f, 0)

    def minor_step(d):
        for st in streams:
            first_got(st, d)
        if d < 4:
            for st in streams:
                first_send(st, d + 1)
            second_first(2 * d - 1)
            second_first(2 * d)
        else:
            second_first(7)

    class Exchange:
        def __init__(self, PB, RB, SND, RCV, ds, dr, ns, nr):
            self.PB, self.RB, self.SND, self.RCV = PB, RB, SND, RCV
            self.ds, self.dr, self.ns, self.nr = ds, dr, ns, nr

        def to_partner(self, k):
            for q in (2, 1, 3, 0):
                b = xm(q)
                put(self.PB.at[k, b * C + co], self.RB.at[k, b], self.ds.at[k, q],
                    self.dr.at[k, q], partner)

        def pair(self, k, q, side):
            b = xm(q)
            return self.PB[k, b * C + c, side].astype(F32) + self.RB[k, b, side].astype(F32)

        def partner_got(self, k, q):
            got(self.RB.at[k, xm(q)], self.ds.at[k, q], self.dr.at[k, q])

        def send(self, k, slot, value, dirn):
            self.SND[k, slot] = value.astype(BF)
            put(self.SND.at[k, slot], self.RCV.at[k, slot], self.ns.at[k, slot],
                self.nr.at[k, slot], at_x(dirn))

        def have(self, k, slot):
            got(self.RCV.at[k, slot], self.ns.at[k, slot], self.nr.at[k, slot])
            return self.RCV[k, slot].astype(F32)

        def far(self, k):
            self.partner_got(k, 2)
            self.send(k, 0, self.pair(k, 2, 0), 1)
            self.send(k, 1, self.pair(k, 2, 1), -1)
            self.partner_got(k, 1)
            self.send(k, 2, self.pair(k, 1, 1), 1)
            self.partner_got(k, 3)
            self.send(k, 3, self.pair(k, 3, 0), -1)

        def grow(self, k):
            self.send(k, 4, self.pair(k, 1, 0) + self.have(k, 0), 1)
            self.send(k, 5, self.pair(k, 3, 1) + self.have(k, 1), -1)

        def total(self, k):
            self.partner_got(k, 0)
            left = self.pair(k, 0, 0) + self.have(k, 3) + self.have(k, 4)
            right = self.pair(k, 0, 1) + self.have(k, 2) + self.have(k, 5)
            return left, right

    class Gather:
        def __init__(self, G, cols, s, r):
            self.G, self.cols, self.s, self.r = G, cols, s, r

        def ref(self, k, q, side, core):
            return self.G.at[xm(q) * C + core, :, self.cols(k, side)]

        def go(self, k, slot, q, side, dev):
            ref = self.ref(k, q, side, c)
            put(ref, ref, self.s.at[k, slot], self.r.at[k, slot], dev)

        def wait(self, k, slot, q, side, core):
            got(self.ref(k, q, side, core), self.s.at[k, slot], self.r.at[k, slot])

        def own(self, k):
            self.go(k, 0, 0, 0, at_x(1))
            self.go(k, 1, 0, 1, at_x(-1))
            self.go(k, 2, 0, 1, at_x(1))
            self.go(k, 3, 0, 0, at_x(-1))
            self.go(k, 6, 0, 0, partner)
            self.go(k, 7, 0, 1, partner)

        def forward(self, k):
            self.wait(k, 0, 3, 0, c)
            self.go(k, 4, 3, 0, at_x(1))
            self.wait(k, 1, 1, 1, c)
            self.go(k, 5, 1, 1, at_x(-1))
            self.go(k, 8, 3, 0, partner)
            self.go(k, 9, 1, 1, partner)

        def forward2(self, k):
            self.wait(k, 2, 3, 1, c)
            self.go(k, 10, 3, 1, partner)
            self.wait(k, 3, 1, 0, c)
            self.go(k, 11, 1, 0, partner)

        def last(self, k):
            self.wait(k, 4, 2, 0, c)
            self.go(k, 12, 2, 0, partner)
            self.wait(k, 5, 2, 1, c)
            self.go(k, 13, 2, 1, partner)

        def finish(self, k):
            for slot, q, side in (
                (6, 0, 0), (7, 0, 1), (8, 3, 0), (9, 1, 1), (10, 3, 1), (11, 1, 0),
                (12, 2, 0), (13, 2, 1),
            ):
                self.wait(k, slot, q, side, co)

    one = Exchange(PB1, RB1, SND1, RCV1, d1s, d1r, n1s, n1r)
    two = Exchange(PB2, RB2, SND2, RCV2, d2s, d2r, n2s, n2r)
    rows = Gather(NALL, lambda k, side: pl.ds(side * 1024, 1024), a1s, a1r)
    pairs = ((0, -1), (1, -2), (2, -3), (3, -4))

    def block_of(k, side):
        return (z + pairs[k][side] + 8) % 8

    def out_cols(k, side):
        return pl.ds(pl.multiple_of(block_of(k, side) * 256, 256), 256)

    done = Gather(out, out_cols, a2s, a2r)

    for st in streams:
        first_send(st, 1)
    second_first(0)

    loads[2].wait()
    a = att[...]
    H1 = 2048 // (2 * NC1)
    for k in range(NC1):
        for side in range(2):
            lo = (2 * k + side) * H1
            p = jnp.dot(a, WO[:, lo:lo + H1], preferred_element_type=F32).astype(BF)
            PB1[k, :, side] = p.reshape(8, 64, H1)
        one.to_partner(k)
    minor_step(1)
    for k in range(NC1):
        one.far(k)
    minor_step(2)
    for k in range(NC1):
        one.grow(k)
    minor_step(3)
    minor_step(4)
    loads[3].wait()
    pump(0, 4)
    for k in range(NC1):
        for side, part in enumerate(one.total(k)):
            lo = (2 * k + side) * H1
            MID[:, lo:lo + H1] = (RES[:, lo:lo + H1].astype(F32) + part).astype(BF).astype(F32)
    mid = MID[...]
    scale = lax.rsqrt(jnp.mean(mid * mid, axis=-1, keepdims=True) + EPS)
    normed = (mid * scale * gain[...]).astype(BF).astype(F32)
    lane = lax.broadcasted_iota(jnp.int32, (64, 128), 1) // 32
    own = NALL.at[x * C + c]
    for yy in range(8):
        for h in range(2):
            got_cols = None
            for q in range(4):
                lo = (4 * h + q) * 256 + (yy // 4) * 128
                piece = normed[:, lo:lo + 128]
                shift = ((q - yy % 4) * 32) % 128
                if shift:
                    piece = pltpu.roll(piece, shift, axis=1)
                got_cols = piece if got_cols is None else jnp.where(lane == q, piece, got_cols)
            own[:, yy * 256 + h * 128:yy * 256 + h * 128 + 128] = got_cols.astype(BF)
    rows.own(0)
    pump(4, 8)
    rows.forward(0)
    rows.forward2(0)
    pump(8, 12)
    rows.last(0)
    rows.finish(0)

    def up_block(off, first):
        q = (y + off + 8) % 8

        def tile(n, _):
            lhs = NALL[:, :, pl.ds(pl.multiple_of(q * 256, 256), 256)].reshape(512, 256)
            rhs = WU[q, :, :, pl.ds(pl.multiple_of(n * 256, 256), 256)].reshape(256, 256)
            d = jnp.dot(lhs, rhs, preferred_element_type=F32)
            if first:
                ACC[n] = d
            else:
                ACC[n] += d
            return 0

        lax.fori_loop(0, 4, tile, 0)

    up_block(0, True)
    up_block(-1, False)
    up_block(1, False)
    pump(12, 16)
    up_block(-2, False)
    up_block(2, False)
    pump(16, 24)
    up_block(-3, False)
    up_block(3, False)
    pump(24, 28)
    up_block(4, False)

    def squared(n, _):
        r = jnp.maximum(ACC[n], 0.0)
        ACT[:, pl.ds(pl.multiple_of(n * 256, 256), 256)] = (r * r).astype(BF)
        return 0

    lax.fori_loop(0, 4, squared, 0)

    def s_down(k):
        for side in range(2):
            w = WD[block_of(k, side)].reshape(256, 1024)
            p = lax.dot_general(
                ACT[...], w, (((1,), (1,)), ((), ())), preferred_element_type=F32
            ).astype(BF)
            PB2[k, :, side] = p.reshape(8, 64, 256)
        two.to_partner(k)

    def s_total(k):
        for side, part in enumerate(two.total(k)):
            cols = out_cols(k, side)
            out[x * C + c, :, cols] = (MID[:, cols] + part).astype(BF)
        done.own(k)

    stages = (
        s_down, two.far, two.grow, s_total, done.forward, done.forward2, done.last, done.finish
    )
    for t in range(NC2 + len(stages) - 1):
        for i, stage in enumerate(stages):
            if 0 <= t - i < NC2:
                stage(t - i)

    for wait in pending:
        wait()

    def sent(m, _):
        for st in streams:
            ref = st[1].at[0, 0]
            rc(ref, ref, g2s.at[st[0], m], g2r.at[st[0], m], st[4]).wait_send()
        return 0

    lax.fori_loop(0, 28, sent, 0)


def layer(att, w_out, resid, n_gain, w_up, wdt):
    rows, width = resid.shape
    vm, hbm = pl.BlockSpec(memory_space=pltpu.VMEM), pl.BlockSpec(memory_space=pl.ANY)
    H1, H2 = 2048 // (2 * NC1), 2048 // (2 * NC2)
    dma = pltpu.SemaphoreType.DMA
    out = pl.pallas_call(
        fused,
        out_shape=jax.ShapeDtypeStruct((8, rows // 8, width), BF),
        in_specs=[vm, hbm, hbm, vm, hbm, hbm],
        out_specs=vm,
        scratch_shapes=[
            pltpu.VMEM((8, 8, 32, 1024), BF),
            pltpu.VMEM((8, 8, 32, 1024), BF),
            pltpu.VMEM((256, 2048), BF),
            pltpu.VMEM((64, 2048), BF),
            pltpu.VMEM((NC1, 8, 2, 64, H1), BF),
            pltpu.VMEM((NC1, 4, 2, 64, H1), BF),
            pltpu.VMEM((NC1, 6, 64, H1), BF),
            pltpu.VMEM((NC1, 6, 64, H1), BF),
            pltpu.VMEM((NC2, 8, 2, 64, H2), BF),
            pltpu.VMEM((NC2, 4, 2, 64, H2), BF),
            pltpu.VMEM((NC2, 6, 64, H2), BF),
            pltpu.VMEM((NC2, 6, 64, H2), BF),
            pltpu.VMEM((8, 64, 2048), BF),
            pltpu.VMEM((64, 2048), F32),
            pltpu.VMEM((4, 512, 256), F32),
            pltpu.VMEM((512, 1024), BF),
            dma((4,)),
            dma((4, 4)), dma((4, 4)),
            dma((4, 28)), dma((4, 28)),
            dma((NC1, 4)), dma((NC1, 4)), dma((NC1, 6)), dma((NC1, 6)),
            dma((NC2, 4)), dma((NC2, 4)), dma((NC2, 6)), dma((NC2, 6)),
            dma((1, 14)), dma((1, 14)), dma((NC2, 14)), dma((NC2, 14)),
        ],
        compiler_params=pltpu.CompilerParams(
            collective_id=0, has_side_effects=True, vmem_limit_bytes=60 * 1024 * 1024
        ),
        name="layer",
    )(att, w_out, resid, n_gain.reshape(1, -1), w_up, wdt)
    return out.reshape(rows, width)


def shards(
    resid, queries, keys, values, documents, q_gain, k_gain, sink, w_out, n_gain, w_up, w_down
):
    rows = resid.shape[0]
    head_size = q_gain.shape[0]
    heads_here = sink.shape[0]
    kv_here = keys.shape[1] // head_size
    group = heads_here // kv_here
    qnorm = rms_scale(queries.reshape(rows, kv_here, group, head_size), q_gain).astype(BF)
    knorm = rms_scale(keys.reshape(rows, kv_here, head_size), k_gain).astype(BF)
    vheads = values.reshape(rows, kv_here, head_size)
    doc_here = documents.astype(BF)
    near_keys, near_values, near_docs = (
        extended(knorm, (("sp", 0),), WINDOW),
        extended(vheads, (("sp", 0),), WINDOW),
        extended(doc_here, (("sp", 0),), WINDOW),
    )
    offset = lax.axis_index("sp") * rows
    total = rows * lax.axis_size("sp")
    query_pos = offset + jnp.arange(rows, dtype=jnp.int32)
    key_pos = offset - WINDOW + jnp.arange(rows + 2 * WINDOW, dtype=jnp.int32)
    distance = key_pos[None, :] - query_pos[:, None]
    allowed = (jnp.abs(distance) <= WINDOW) & (key_pos[None, :] >= 0) & (key_pos[None, :] < total)
    allowed = allowed & (near_docs[None, :] == doc_here[:, None])
    heads_all = heads_here * lax.axis_size("tp")
    first_head = (lax.axis_index("tp") * heads_here).astype(F32)
    slopes = jnp.exp2(-8.0 * (first_head + jnp.arange(heads_here, dtype=F32) + 1.0) / heads_all)
    slopes = slopes.reshape(kv_here, group)
    sink_f = sink.reshape(kv_here, group)
    scores = jnp.einsum(
        "rkgd,skd->kgrs", qnorm, near_keys, preferred_element_type=F32
    ) * head_size ** (-0.5)
    scores = scores - slopes[:, :, None, None] * jnp.abs(distance).astype(F32)[None, None]
    scores = jnp.where(allowed[None, None], scores, F32(-1e30))
    highest = jnp.maximum(jnp.max(scores, axis=-1), sink_f[:, :, None])
    weights = jnp.exp(scores - highest[..., None])
    denom = jnp.sum(weights, axis=-1) + jnp.exp(sink_f[:, :, None] - highest)
    summed = jnp.einsum(
        "kgrs,skd->rkgd", weights.astype(BF), near_values, preferred_element_type=F32
    )
    attended = (
        (summed / denom.transpose(2, 0, 1)[..., None])
        .astype(BF)
        .reshape(rows, heads_here * head_size)
    )
    return layer(attended, w_out, resid, n_gain, w_up, w_down.T)


def solution(mesh):
    placed = (
        P("sp", None), P("sp", "tp"), P("sp", "tp"), P("sp", "tp"), P("sp"), P(), P(),
        P("tp"), P("tp", None), P(), P("sp", "tp"), P("tp", "sp"),
    )
    return jax.shard_map(
        shards, mesh=mesh, in_specs=placed, out_specs=P("sp", None), check_vma=False
    )
```

```python
import functools

import jax
import jax.numpy as jnp
from jax import lax
from jax.experimental import pallas as pl
from jax.experimental.pallas import tpu as pltpu
from jax.sharding import PartitionSpec as P

EPS = 1e-06
Z, Y, X, C = 8, 8, 4, 2
MESH = pl.DeviceIdType.MESH
BF, F32 = jnp.bfloat16, jnp.float32
NC1, NC2 = 2, 4


def fused(
    q_h, k_h, v_h, doc_h, qg, kg, sink, wout_h, resid_h, gain, wup_h, wdt_h, out,
    QX, KX, VX, DX, KN, ATT, WU, WD, WO, RES, PB1, RB1, SND1, RCV1, PB2, RB2, SND2, RCV2, NALL, MID, ACC, ACT,
    loc, hs, hr, g1s, g1r, g2s, g2r, d1s, d1r, n1s, n1r, d2s, d2r, n2s, n2r, a1s, a1r, a2s, a2r,
):
    sp, tp = lax.axis_index("sp"), lax.axis_index("tp")
    z, y = sp // Y, sp % Y
    x, c = tp // C, tp % C
    co = 1 - c

    def at_z(s):
        return (((z + s + Z) % Z) * Y + y, tp)

    def at_y(s):
        return (z * Y + (y + s + Y) % Y, tp)

    def xm(s):
        return (x + s + X) % X

    def at_x(s):
        return (sp, xm(s) * C + c)

    partner = (sp, x * C + co)
    pending = []

    def rc(src, dst, ss, rs, dev):
        return pltpu.make_async_remote_copy(
            src_ref=src, dst_ref=dst, send_sem=ss, recv_sem=rs, device_id=dev, device_id_type=MESH
        )

    def put(src, dst, ss, rs, dev):
        rc(src, dst, ss, rs, dev).start()
        pending.append(lambda: rc(src, dst, ss, rs, dev).wait_send())

    def got(ref, ss, rs):
        rc(ref, ref, ss, rs, partner).wait_recv()

    loads = [
        pltpu.make_async_copy(wup_h, WU.at[y, z], loc.at[0]),
        pltpu.make_async_copy(k_h, KX.at[:, pl.ds(128, 512)], loc.at[1]),
        pltpu.make_async_copy(v_h, VX.at[:, pl.ds(128, 512)], loc.at[2]),
        pltpu.make_async_copy(doc_h, DX.at[pl.ds(1, 4)], loc.at[3]),
        pltpu.make_async_copy(wdt_h, WD.at[z, y], loc.at[4]),
        pltpu.make_async_copy(q_h, QX, loc.at[5]),
        pltpu.make_async_copy(wout_h, WO, loc.at[6]),
        pltpu.make_async_copy(
            resid_h.at[pl.ds(pl.multiple_of(tp * 64, 64), 64)], RES, loc.at[7]
        ),
    ]
    for copy in loads:
        copy.start()
    barrier = pltpu.get_barrier_semaphore()
    after, before = ((sp + 1) % (Z * Y), tp), ((sp + Z * Y - 1) % (Z * Y), tp)
    near = [at_z(1), at_z(-1), at_y(1), at_y(-1), at_x(1), at_x(-1), partner, after, before]
    for dev in near:
        pl.semaphore_signal(barrier, inc=1, device_id=dev, device_id_type=MESH)
    for copy in loads[:5]:
        copy.wait()
    pl.semaphore_wait(barrier, len(near))

    streams = []
    for w, (buf, ma, mi, dma, dmi) in enumerate(
        ((WU, y, z, at_y, at_z), (WD, z, y, at_z, at_y))
    ):
        for e, s in enumerate((1, -1)):
            streams.append((2 * w + e, buf, ma, mi, dma(s), dmi(s), s, e))

    def minor_off(j):
        return jnp.where(j % 2 == 1, -((j + 1) // 2), j // 2)

    def first_ref(st, d, at_me):
        i, buf, ma, mi, _, _, s, e = st
        dist = d if at_me else d - 1
        ref = buf.at[ma, (mi - s * dist + 8) % 8]
        return ref.at[pl.ds(16 * e, 16)] if d == 4 else ref

    def first_send(st, d):
        i, buf, ma, mi, _, dev, s, e = st
        src = first_ref(st, d, False)
        put(src, src, g1s.at[i, d - 1], g1r.at[i, d - 1], dev)

    def first_got(st, d):
        i = st[0]
        got(first_ref(st, d, True), g1s.at[i, d - 1], g1r.at[i, d - 1])

    def second_copy(st, d, j, m):
        i, buf, ma, mi, dev, _, s, e = st
        src = buf.at[(ma - s * (d - 1) + 8) % 8, (mi + minor_off(j) + 8) % 8]
        return rc(src, src, g2s.at[i, m], g2r.at[i, m], dev)

    def second_got(st, d, j, m):
        i, buf, ma, mi, dev, _, s, e = st
        ref = buf.at[(ma - s * d + 16) % 8, (mi + minor_off(j) + 8) % 8]
        got(ref, g2s.at[i, m], g2r.at[i, m])

    def second_first(j):
        for st in streams:
            second_copy(st, 1, j, j).start()

    def pump(lo, hi):
        def both(m, _):
            d, j = m // 8 + 1, m % 8
            for st in streams:
                second_got(st, d, j, m)
                second_copy(st, d + 1, j, m + 8).start()
            return 0

        def half(m, _, es):
            d, j = m // 8 + 1, m % 8
            for st in streams:
                second_got(st, d, j, m)
                if st[7] in es:
                    second_copy(st, 4, j, m + 8 - 4 * st[7]).start()
            return 0

        def last(m, _):
            for st in streams:
                second_got(st, 4, m - 24 + 4 * st[7], m)
            return 0

        for a, b, f in (
            (0, 16, both),
            (16, 20, functools.partial(half, es=(0,))),
            (20, 24, functools.partial(half, es=(1,))),
            (24, 28, last),
        ):
            a, b = max(a, lo), min(b, hi)
            if a < b:
                lax.fori_loop(a, b, f, 0)

    def minor_step(d):
        for st in streams:
            first_got(st, d)
        if d < 4:
            for st in streams:
                first_send(st, d + 1)
            second_first(2 * d - 1)
            second_first(2 * d)
        else:
            second_first(7)

    class Exchange:
        def __init__(self, PB, RB, SND, RCV, ds, dr, ns, nr):
            self.PB, self.RB, self.SND, self.RCV = PB, RB, SND, RCV
            self.ds, self.dr, self.ns, self.nr = ds, dr, ns, nr

        def to_partner(self, k):
            for q in (2, 1, 3, 0):
                b = xm(q)
                put(self.PB.at[k, b * C + co], self.RB.at[k, b], self.ds.at[k, q],
                    self.dr.at[k, q], partner)

        def pair(self, k, q, side):
            b = xm(q)
            return self.PB[k, b * C + c, side].astype(F32) + self.RB[k, b, side].astype(F32)

        def partner_got(self, k, q):
            got(self.RB.at[k, xm(q)], self.ds.at[k, q], self.dr.at[k, q])

        def send(self, k, slot, value, dirn):
            self.SND[k, slot] = value.astype(BF)
            put(self.SND.at[k, slot], self.RCV.at[k, slot], self.ns.at[k, slot],
                self.nr.at[k, slot], at_x(dirn))

        def have(self, k, slot):
            got(self.RCV.at[k, slot], self.ns.at[k, slot], self.nr.at[k, slot])
            return self.RCV[k, slot].astype(F32)

        def far(self, k):
            self.partner_got(k, 2)
            self.send(k, 0, self.pair(k, 2, 0), 1)
            self.send(k, 1, self.pair(k, 2, 1), -1)
            self.partner_got(k, 1)
            self.send(k, 2, self.pair(k, 1, 1), 1)
            self.partner_got(k, 3)
            self.send(k, 3, self.pair(k, 3, 0), -1)

        def grow(self, k):
            self.send(k, 4, self.pair(k, 1, 0) + self.have(k, 0), 1)
            self.send(k, 5, self.pair(k, 3, 1) + self.have(k, 1), -1)

        def total(self, k):
            self.partner_got(k, 0)
            left = self.pair(k, 0, 0) + self.have(k, 3) + self.have(k, 4)
            right = self.pair(k, 0, 1) + self.have(k, 2) + self.have(k, 5)
            return left, right

    class Gather:
        def __init__(self, G, cols, s, r):
            self.G, self.cols, self.s, self.r = G, cols, s, r

        def ref(self, k, q, side, core):
            return self.G.at[xm(q) * C + core, :, self.cols(k, side)]

        def go(self, k, slot, q, side, dev):
            ref = self.ref(k, q, side, c)
            put(ref, ref, self.s.at[k, slot], self.r.at[k, slot], dev)

        def wait(self, k, slot, q, side, core):
            got(self.ref(k, q, side, core), self.s.at[k, slot], self.r.at[k, slot])

        def own(self, k):
            self.go(k, 0, 0, 0, at_x(1))
            self.go(k, 1, 0, 1, at_x(-1))
            self.go(k, 2, 0, 1, at_x(1))
            self.go(k, 3, 0, 0, at_x(-1))
            self.go(k, 6, 0, 0, partner)
            self.go(k, 7, 0, 1, partner)

        def forward(self, k):
            self.wait(k, 0, 3, 0, c)
            self.go(k, 4, 3, 0, at_x(1))
            self.wait(k, 1, 1, 1, c)
            self.go(k, 5, 1, 1, at_x(-1))
            self.go(k, 8, 3, 0, partner)
            self.go(k, 9, 1, 1, partner)

        def forward2(self, k):
            self.wait(k, 2, 3, 1, c)
            self.go(k, 10, 3, 1, partner)
            self.wait(k, 3, 1, 0, c)
            self.go(k, 11, 1, 0, partner)

        def last(self, k):
            self.wait(k, 4, 2, 0, c)
            self.go(k, 12, 2, 0, partner)
            self.wait(k, 5, 2, 1, c)
            self.go(k, 13, 2, 1, partner)

        def finish(self, k):
            for slot, q, side in (
                (6, 0, 0), (7, 0, 1), (8, 3, 0), (9, 1, 1), (10, 3, 1), (11, 1, 0),
                (12, 2, 0), (13, 2, 1),
            ):
                self.wait(k, slot, q, side, co)

    one = Exchange(PB1, RB1, SND1, RCV1, d1s, d1r, n1s, n1r)
    two = Exchange(PB2, RB2, SND2, RCV2, d2s, d2r, n2s, n2r)
    rows = Gather(NALL, lambda k, side: pl.ds(side * 1024, 1024), a1s, a1r)
    pairs = ((0, -1), (1, -2), (2, -3), (3, -4))

    def block_of(k, side):
        return (z + pairs[k][side] + 8) % 8

    def out_cols(k, side):
        return pl.ds(pl.multiple_of(block_of(k, side) * 256, 256), 256)

    done = Gather(out, out_cols, a2s, a2r)

    halo = []
    for i, ref in enumerate((KX, VX, DX)):
        part = [
            ref.at[pl.ds(n, 1)] if i == 2 else ref.at[:, pl.ds(128 * n, 128)] for n in range(6)
        ]
        put(part[4], part[0], hs.at[0, i], hr.at[0, i], after)
        put(part[1], part[5], hs.at[1, i], hr.at[1, i], before)
        halo.append((part[0], part[5]))

    def halo_got(side):
        for i in range(3):
            got(halo[i][side], hs.at[side, i], hr.at[side, i])

    for st in streams:
        first_send(st, 1)
    second_first(0)

    def head_norm(rows_, gain_, ones):
        wide = rows_.astype(F32)
        square = wide * wide
        high = square.astype(BF)
        low = (square - high.astype(F32)).astype(BF)
        mean = (
            jnp.dot(high, ones, preferred_element_type=F32)
            + jnp.dot(low, ones, preferred_element_type=F32)
        ) * (1.0 / 64)
        return (wide * lax.rsqrt(mean + EPS) * gain_).astype(BF)

    def iotas(rows_, cols_):
        return [lax.broadcasted_iota(jnp.int32, (rows_, cols_), i) for i in range(2)]

    r64, c64 = iotas(64, 64)
    kgain = jnp.sum(jnp.where(r64 == c64, kg[...], 0.0), axis=1, keepdims=True)
    r256, c256 = iotas(256, 256)
    ones256 = (r256 // 64 == c256 // 64).astype(BF)

    def key_norm(lo, n):
        wide = KX[:, lo:lo + n].astype(F32)
        mean = jnp.mean(wide * wide, axis=0, keepdims=True)
        KN[:, lo:lo + n] = (wide * lax.rsqrt(mean + EPS) * kgain).astype(BF)

    key_norm(128, 512)
    loads[5].wait()
    qgain = jnp.concatenate([qg[...]] * 4, axis=1)
    heads = [
        jnp.exp2(jnp.full((1, 1), (tp * 4 + h + 1).astype(F32) * -0.25)) for h in range(4)
    ]
    row = lax.broadcasted_iota(jnp.int32, (128, 128), 0)
    col = lax.broadcasted_iota(jnp.int32, (128, 128), 1)
    span = jnp.abs(
        lax.broadcasted_iota(jnp.int32, (128, 384), 1) - 128
        - lax.broadcasted_iota(jnp.int32, (128, 384), 0)
    ).astype(F32)

    def attend(b):
        qn = head_norm(QX[128 * b:128 * b + 128], qgain, ones256)
        kb, vb = KN[:, 128 * b:128 * b + 384], VX[:, 128 * b:128 * b + 384]
        docs = [DX[b + i].astype(F32) for i in range(3)]
        mine = jnp.transpose(jnp.broadcast_to(docs[1], (128, 128)))
        if b == 0:
            docs[0] = jnp.where(sp == 0, -1.0, docs[0])
        if b == 3:
            docs[2] = jnp.where(sp == Z * Y - 1, -1.0, docs[2])
        allowed = jnp.concatenate(
            [(mine == docs[0]) & (col >= row), mine == docs[1], (mine == docs[2]) & (col <= row)],
            axis=1,
        )
        outs = []
        for h in range(4):
            score = jnp.dot(qn[:, 64 * h:64 * h + 64], kb, preferred_element_type=F32)
            score = score * 0.125 - heads[h] * span
            score = jnp.where(allowed, score, -1e30)
            top = jnp.maximum(jnp.max(score, axis=1, keepdims=True), sink[h])
            p = jnp.exp(score - top)
            denom = jnp.sum(p, axis=1, keepdims=True) + jnp.exp(sink[h] - top)
            mixed = lax.dot_general(
                p.astype(BF), vb, (((1,), (1,)), ((), ())), preferred_element_type=F32
            )
            outs.append((mixed / denom).astype(BF))
        ATT[128 * b:128 * b + 128] = jnp.concatenate(outs, axis=1)

    attend(1)
    minor_step(1)
    attend(2)
    halo_got(0)
    key_norm(0, 128)
    attend(0)
    minor_step(2)
    halo_got(1)
    key_norm(640, 128)
    attend(3)
    loads[6].wait()
    a = ATT[...]
    H1 = 2048 // (2 * NC1)
    for k in range(NC1):
        for side in range(2):
            lo = (2 * k + side) * H1
            p = jnp.dot(a, WO[:, lo:lo + H1], preferred_element_type=F32).astype(BF)
            PB1[k, :, side] = p.reshape(8, 64, H1)
        one.to_partner(k)
    minor_step(3)
    for k in range(NC1):
        one.far(k)
    for k in range(NC1):
        one.grow(k)
    minor_step(4)
    loads[7].wait()
    pump(0, 4)
    for k in range(NC1):
        for side, part in enumerate(one.total(k)):
            lo = (2 * k + side) * H1
            MID[:, lo:lo + H1] = (RES[:, lo:lo + H1].astype(F32) + part).astype(BF).astype(F32)
    mid = MID[...]
    scale = lax.rsqrt(jnp.mean(mid * mid, axis=-1, keepdims=True) + EPS)
    normed = (mid * scale * gain[...]).astype(BF).astype(F32)
    lane = lax.broadcasted_iota(jnp.int32, (64, 128), 1) // 32
    own = NALL.at[x * C + c]
    for yy in range(8):
        for h in range(2):
            got_cols = None
            for q in range(4):
                lo = (4 * h + q) * 256 + (yy // 4) * 128
                piece = normed[:, lo:lo + 128]
                shift = ((q - yy % 4) * 32) % 128
                if shift:
                    piece = pltpu.roll(piece, shift, axis=1)
                got_cols = piece if got_cols is None else jnp.where(lane == q, piece, got_cols)
            own[:, yy * 256 + h * 128:yy * 256 + h * 128 + 128] = got_cols.astype(BF)
    rows.own(0)
    pump(4, 8)
    rows.forward(0)
    rows.forward2(0)
    pump(8, 12)
    rows.last(0)
    rows.finish(0)

    def up_block(off, first):
        q = (y + off + 8) % 8

        def tile(n, _):
            lhs = NALL[:, :, pl.ds(pl.multiple_of(q * 256, 256), 256)].reshape(512, 256)
            rhs = WU[q, :, :, pl.ds(pl.multiple_of(n * 256, 256), 256)].reshape(256, 256)
            d = jnp.dot(lhs, rhs, preferred_element_type=F32)
            if first:
                ACC[n] = d
            else:
                ACC[n] += d
            return 0

        lax.fori_loop(0, 4, tile, 0)

    up_block(0, True)
    up_block(-1, False)
    up_block(1, False)
    pump(12, 16)
    up_block(-2, False)
    up_block(2, False)
    pump(16, 24)
    up_block(-3, False)
    up_block(3, False)
    pump(24, 28)
    up_block(4, False)

    def squared(n, _):
        r = jnp.maximum(ACC[n], 0.0)
        ACT[:, pl.ds(pl.multiple_of(n * 256, 256), 256)] = (r * r).astype(BF)
        return 0

    lax.fori_loop(0, 4, squared, 0)

    def s_down(k):
        for side in range(2):
            w = WD[block_of(k, side)].reshape(256, 1024)
            p = lax.dot_general(
                ACT[...], w, (((1,), (1,)), ((), ())), preferred_element_type=F32
            ).astype(BF)
            PB2[k, :, side] = p.reshape(8, 64, 256)
        two.to_partner(k)

    def s_total(k):
        for side, part in enumerate(two.total(k)):
            cols = out_cols(k, side)
            out[x * C + c, :, cols] = (MID[:, cols] + part).astype(BF)
        done.own(k)

    stages = (
        s_down, two.far, two.grow, s_total, done.forward, done.forward2, done.last, done.finish
    )
    for t in range(NC2 + len(stages) - 1):
        for i, stage in enumerate(stages):
            if 0 <= t - i < NC2:
                stage(t - i)

    for wait in pending:
        wait()

    def sent(m, _):
        for st in streams:
            ref = st[1].at[0, 0]
            rc(ref, ref, g2s.at[st[0], m], g2r.at[st[0], m], st[4]).wait_send()
        return 0

    lax.fori_loop(0, 28, sent, 0)


def shards(
    resid, queries, keys, values, documents, q_gain, k_gain, sink, w_out, n_gain, w_up, w_down
):
    rows, width = resid.shape
    vm, sm = pl.BlockSpec(memory_space=pltpu.VMEM), pl.BlockSpec(memory_space=pltpu.SMEM)
    hbm = pl.BlockSpec(memory_space=pltpu.HBM)
    H1, H2 = 2048 // (2 * NC1), 2048 // (2 * NC2)
    dma = pltpu.SemaphoreType.DMA
    out = pl.pallas_call(
        fused,
        out_shape=jax.ShapeDtypeStruct((8, rows // 8, width), BF),
        in_specs=[hbm, hbm, hbm, hbm, vm, vm, sm, hbm, hbm, vm, hbm, hbm],
        out_specs=vm,
        scratch_shapes=[
            pltpu.VMEM((512, 256), BF),
            pltpu.VMEM((64, 768), BF),
            pltpu.VMEM((64, 768), BF),
            pltpu.VMEM((6, 1, 128), jnp.int32),
            pltpu.VMEM((64, 768), BF),
            pltpu.VMEM((512, 256), BF),
            pltpu.VMEM((8, 8, 32, 1024), BF),
            pltpu.VMEM((8, 8, 32, 1024), BF),
            pltpu.VMEM((256, 2048), BF),
            pltpu.VMEM((64, 2048), BF),
            pltpu.VMEM((NC1, 8, 2, 64, H1), BF),
            pltpu.VMEM((NC1, 4, 2, 64, H1), BF),
            pltpu.VMEM((NC1, 6, 64, H1), BF),
            pltpu.VMEM((NC1, 6, 64, H1), BF),
            pltpu.VMEM((NC2, 8, 2, 64, H2), BF),
            pltpu.VMEM((NC2, 4, 2, 64, H2), BF),
            pltpu.VMEM((NC2, 6, 64, H2), BF),
            pltpu.VMEM((NC2, 6, 64, H2), BF),
            pltpu.VMEM((8, 64, 2048), BF),
            pltpu.VMEM((64, 2048), F32),
            pltpu.VMEM((4, 512, 256), F32),
            pltpu.VMEM((512, 1024), BF),
            dma((8,)), dma((2, 3)), dma((2, 3)),
            dma((4, 4)), dma((4, 4)),
            dma((4, 28)), dma((4, 28)),
            dma((NC1, 4)), dma((NC1, 4)), dma((NC1, 6)), dma((NC1, 6)),
            dma((NC2, 4)), dma((NC2, 4)), dma((NC2, 6)), dma((NC2, 6)),
            dma((1, 14)), dma((1, 14)), dma((NC2, 14)), dma((NC2, 14)),
        ],
        compiler_params=pltpu.CompilerParams(
            collective_id=0, has_side_effects=True, vmem_limit_bytes=60 * 1024 * 1024
        ),
        name="layer",
    )(
        queries, keys.T, values.T, documents.reshape(4, 1, 128), q_gain.reshape(1, -1),
        k_gain.reshape(1, -1), sink, w_out, resid, n_gain.reshape(1, -1), w_up, w_down.T,
    )
    return out.reshape(rows, width)


def solution(mesh):
    placed = (
        P("sp", None), P("sp", "tp"), P("sp", "tp"), P("sp", "tp"), P("sp"), P(), P(),
        P("tp"), P("tp", None), P(), P("sp", "tp"), P("tp", "sp"),
    )
    return jax.shard_map(
        shards, mesh=mesh, in_specs=placed, out_specs=P("sp", None), check_vma=False
    )
```

```python
import functools

import jax
import jax.numpy as jnp
from jax import lax
from jax.experimental import pallas as pl
from jax.experimental.pallas import tpu as pltpu
from jax.sharding import PartitionSpec as P

EPS = 1e-06
Z, Y, X, C = 8, 8, 4, 2
MESH = pl.DeviceIdType.MESH
BF, F32 = jnp.bfloat16, jnp.float32
NC1, NC2 = 2, 4


def fused(
    q_h, k_h, v_h, doc_h, qg, kg, sink, wout_h, resid_h, gain, wup_h, wdt_h, out,
    QX, KX, VX, DX, KN, ATT, WU, WD, WO, RES, PB1, RB1, SND1, RCV1, PB2, RB2, SND2, RCV2, NALL, MID, ACT, OWN,
    loc, left, hr, gr, rr, fr, er, d1r, n1r, d2r, n2r, a1r, a2r,
):
    sp, tp = lax.axis_index("sp"), lax.axis_index("tp")
    z, y = sp // Y, sp % Y
    x, c = tp // C, tp % C
    co = 1 - c

    def at_z(s):
        return (((z + s + Z) % Z) * Y + y, tp)

    def at_y(s):
        return (z * Y + (y + s + Y) % Y, tp)

    def xm(s):
        return (x + s + X) % X

    def at_x(s):
        return (sp, xm(s) * C + c)

    partner = (sp, x * C + co)

    def rc(src, dst, ss, rs, dev):
        return pltpu.make_async_remote_copy(
            src_ref=src, dst_ref=dst, send_sem=ss, recv_sem=rs, device_id=dev, device_id_type=MESH
        )

    def put(src, dst, ss, rs, dev):
        rc(src, dst, ss, rs, dev).start()

    def got(ref, rs):
        rc(ref, ref, left.at[0], rs, partner).wait_recv()

    loads = [
        pltpu.make_async_copy(wup_h, WU.at[z, y], loc.at[0]),
        pltpu.make_async_copy(k_h, KX.at[:, pl.ds(128, 512)], loc.at[1]),
        pltpu.make_async_copy(v_h, VX.at[:, pl.ds(128, 512)], loc.at[2]),
        pltpu.make_async_copy(doc_h, DX.at[pl.ds(1, 4)], loc.at[3]),
        pltpu.make_async_copy(wdt_h, WD.at[z, y], loc.at[4]),
        pltpu.make_async_copy(q_h, QX, loc.at[5]),
        pltpu.make_async_copy(wout_h, WO, loc.at[6]),
        pltpu.make_async_copy(
            resid_h.at[pl.ds(pl.multiple_of(tp * 64, 64), 64)], RES, loc.at[7]
        ),
    ]
    for copy in loads:
        copy.start()
    barrier = pltpu.get_barrier_semaphore()
    after, before = ((sp + 1) % (Z * Y), tp), ((sp + Z * Y - 1) % (Z * Y), tp)
    near = [at_z(1), at_z(-1), at_y(1), at_y(-1), at_x(1), at_x(-1), partner, after, before]
    for dev in near:
        pl.semaphore_signal(barrier, inc=1, device_id=dev, device_id_type=MESH)
    pl.semaphore_wait(barrier, len(near))

    pieces = ((WU, 0, 512, "z"), (WU, 512, 512, "y"))
    ways = ((0, 1), (1, -1))

    def shard_ref(p, e, major, minor, half):
        buf, lo, n, axis = pieces[p]
        zz, yy = ((z + minor + 16) % 8, (y + major + 16) % 8)
        if axis == "y":
            zz, yy = ((z + major + 16) % 8, (y + minor + 16) % 8)
        rows_ = pl.ds(16 * e, 16) if half else slice(None)
        return buf.at[zz, yy, rows_, pl.ds(lo, n)]

    def ring_send(p, d):
        for e, s in ways:
            src = shard_ref(p, e, 0, -s * (d - 1), d == 4)
            dev = at_z(s) if pieces[p][3] == "z" else at_y(s)
            put(src, src, left.at[0], rr.at[p, e, d - 1], dev)

    def minor_off(j):
        return jnp.where(j % 2 == 1, -((j + 1) // 2), j // 2)

    def row_copy(p, e, s, d, j, m):
        src = shard_ref(p, e, -s * (d - 1), minor_off(j), False)
        dev = at_y(s) if pieces[p][3] == "z" else at_z(s)
        return rc(src, src, left.at[1], gr.at[p, e, m], dev)

    def row_got(p, e, s, d, j, m):
        got(shard_ref(p, e, -s * d, minor_off(j), False), gr.at[p, e, m])

    def row_send(p, j):
        for e, s in ways:
            row_copy(p, e, s, 1, j, j).start()

    def ring_step(ps, d):
        for p in ps:
            for e, s in ways:
                got(shard_ref(p, e, 0, -s * d, d == 4), rr.at[p, e, d - 1])
            if d < 4:
                ring_send(p, d + 1)
        for j in (2 * d - 1, 2 * d):
            if j < 8:
                for p in ps:
                    row_send(p, j)

    def pump(ps, lo, hi):
        def on(m, _):
            d, j = m // 8 + 1, m % 8
            for p in ps:
                for e, s in ways:
                    row_got(p, e, s, d, j, m)
                    row_copy(p, e, s, d + 1, j, m + 8).start()
            return 0

        def half(m, _, to):
            for p in ps:
                for e, s in ways:
                    row_got(p, e, s, 3, m - 16, m)
                    if e == to:
                        row_copy(p, e, s, 4, m - 16, m + 8 - 4 * e).start()
            return 0

        def last(m, _):
            for p in ps:
                for e, s in ways:
                    row_got(p, e, s, 4, m - 24 + 4 * e, m)
            return 0

        for a, b, f in (
            (0, 16, on),
            (16, 20, functools.partial(half, to=0)),
            (20, 24, functools.partial(half, to=1)),
            (24, 28, last),
        ):
            a, b = max(a, lo), min(b, hi)
            if b - a == 1:
                f(a, 0)
            elif a < b:
                lax.fori_loop(a, b, f, 0)

    ring_base = (0, -3, 3, 4)

    def down_ref(e, dz, dy, half):
        ref = WD.at[(z + dz + 16) % 8, (y + dy + 16) % 8]
        return ref.at[pl.ds(16 * e, 16)] if half else ref

    def loop_send(r, d):
        for e, s in ways:
            src = down_ref(e, ring_base[r], -s * (d - 1), d == 4)
            put(src, src, left.at[2], er.at[r, e, d - 1], at_y(s))

    def loop_step(r, d):
        for e, s in ways:
            got(down_ref(e, ring_base[r], -s * d, d == 4), er.at[r, e, d - 1])
        if d < 4:
            loop_send(r, d + 1)

    def down_copy(e, s, d, j):
        m = 17 if d == 4 else (d - 1) * 8 + j
        src = down_ref(e, -s * (d - 1), minor_off(j), d == 4)
        return rc(src, src, left.at[3], fr.at[e, m], at_z(s))

    def down_send(d, lo, hi):
        for j in range(lo, hi):
            for e, s in ways:
                down_copy(e, s, d, j).start()

    def down_got(d, j):
        m = 17 if d == 4 else (d - 1) * 8 + j
        for e, s in ways:
            got(down_ref(e, -s * d, minor_off(j), d == 4), fr.at[e, m])

    def chain(d):
        down_got(d, 0)
        if d < 4:
            down_send(d + 1, 0, 1)

    def pass_on(lo, hi):
        def one_row(j, _):
            down_got(1, j)
            for e, s in ways:
                down_copy(e, s, 2, j).start()
            return 0

        lax.fori_loop(lo, hi, one_row, 0)

    def take(lo, hi):
        def one_row(j, _):
            down_got(2, j)
            return 0

        lax.fori_loop(lo, hi, one_row, 0)

    class Exchange:
        def __init__(self, PB, RB, SND, RCV, ds, dr, ns, nr):
            self.PB, self.RB, self.SND, self.RCV = PB, RB, SND, RCV
            self.ds, self.dr, self.ns, self.nr = ds, dr, ns, nr

        def to_partner(self, k):
            for q in (2, 1, 3, 0):
                b = xm(q)
                put(self.PB.at[k, b * C + co], self.RB.at[k, b], self.ds, self.dr.at[k, q],
                    partner)

        def pair(self, k, q, side):
            b = xm(q)
            return self.PB[k, b * C + c, side].astype(F32) + self.RB[k, b, side].astype(F32)

        def partner_got(self, k, q):
            got(self.RB.at[k, xm(q)], self.dr.at[k, q])

        def send(self, k, slot, value, dirn):
            self.SND[k, slot] = value.astype(BF)
            put(self.SND.at[k, slot], self.RCV.at[k, slot], self.ns, self.nr.at[k, slot],
                at_x(dirn))

        def have(self, k, slot):
            got(self.RCV.at[k, slot], self.nr.at[k, slot])
            return self.RCV[k, slot].astype(F32)

        def far(self, k):
            self.partner_got(k, 2)
            self.send(k, 0, self.pair(k, 2, 0), 1)
            self.send(k, 1, self.pair(k, 2, 1), -1)
            self.partner_got(k, 1)
            self.send(k, 2, self.pair(k, 1, 1), 1)
            self.partner_got(k, 3)
            self.send(k, 3, self.pair(k, 3, 0), -1)

        def grow(self, k):
            self.send(k, 4, self.pair(k, 1, 0) + self.have(k, 0), 1)
            self.send(k, 5, self.pair(k, 3, 1) + self.have(k, 1), -1)

        def total(self, k):
            self.partner_got(k, 0)
            left = self.pair(k, 0, 0) + self.have(k, 3) + self.have(k, 4)
            right = self.pair(k, 0, 1) + self.have(k, 2) + self.have(k, 5)
            return left, right

    class Gather:
        def __init__(self, G, part, mine, s, r):
            self.G, self.part, self.mine, self.s, self.r = G, part, mine, s, r

        def ref(self, k, q, side, core):
            return self.G.at[(xm(q) * C + core, *self.part(k, side))]

        def go(self, k, slot, q, side, dev):
            ref = self.ref(k, q, side, c)
            src = self.mine.at[self.part(k, side)] if q == 0 else ref
            put(src, ref, self.s, self.r.at[k, slot], dev)

        def wait(self, k, slot, q, side, core):
            got(self.ref(k, q, side, core), self.r.at[k, slot])

        def own(self, k):
            self.go(k, 0, 0, 0, at_x(1))
            self.go(k, 1, 0, 1, at_x(-1))
            self.go(k, 2, 0, 1, at_x(1))
            self.go(k, 3, 0, 0, at_x(-1))
            self.go(k, 6, 0, 0, partner)
            self.go(k, 7, 0, 1, partner)

        def forward(self, k):
            self.wait(k, 0, 3, 0, c)
            self.go(k, 4, 3, 0, at_x(1))
            self.wait(k, 1, 1, 1, c)
            self.go(k, 5, 1, 1, at_x(-1))
            self.go(k, 8, 3, 0, partner)
            self.go(k, 9, 1, 1, partner)

        def forward2(self, k):
            self.wait(k, 2, 3, 1, c)
            self.go(k, 10, 3, 1, partner)
            self.wait(k, 3, 1, 0, c)
            self.go(k, 11, 1, 0, partner)

        def last(self, k):
            self.wait(k, 4, 2, 0, c)
            self.go(k, 12, 2, 0, partner)
            self.wait(k, 5, 2, 1, c)
            self.go(k, 13, 2, 1, partner)

        def finish(self, k):
            for slot, q, side in (
                (6, 0, 0), (7, 0, 1), (8, 3, 0), (9, 1, 1), (10, 3, 1), (11, 1, 0),
                (12, 2, 0), (13, 2, 1),
            ):
                self.wait(k, slot, q, side, co)

    one = Exchange(PB1, RB1, SND1, RCV1, left.at[4], d1r, left.at[5], n1r)
    two = Exchange(PB2, RB2, SND2, RCV2, left.at[6], d2r, left.at[7], n2r)
    rows = Gather(
        NALL, lambda k, side: (pl.ds(32 * k, 32), pl.ds(side * 1024, 1024)), NALL.at[x * C + c],
        left.at[8], a1r,
    )
    pairs = ((0, -1), (1, -3), (3, 4), (2, -2))

    def block_of(k, side):
        return (z + pairs[k][side] + 8) % 8

    def out_cols(k, side):
        return pl.ds(pl.multiple_of(block_of(k, side) * 256, 256), 256)

    done = Gather(out, lambda k, side: (slice(None), out_cols(k, side)), OWN, left.at[9], a2r)

    loads[0].wait()
    ring_send(0, 1)
    ring_send(1, 1)
    for copy in loads[1:4]:
        copy.wait()
    halo = []
    for i, ref in enumerate((KX, VX, DX)):
        part = [
            ref.at[pl.ds(n, 1)] if i == 2 else ref.at[:, pl.ds(128 * n, 128)] for n in range(6)
        ]
        put(part[4], part[0], left.at[10 + i], hr.at[0, i], after)
        put(part[1], part[5], left.at[10 + i], hr.at[1, i], before)
        halo.append((part[0], part[5]))

    row_send(0, 0)
    row_send(1, 0)

    def halo_got(side):
        for i in range(3):
            got(halo[i][side], hr.at[side, i])

    loads[4].wait()
    loop_send(0, 1)
    down_send(1, 0, 1)

    def head_norm(rows_, gain_, ones):
        wide = rows_.astype(F32)
        square = wide * wide
        high = square.astype(BF)
        low = (square - high.astype(F32)).astype(BF)
        mean = (
            jnp.dot(high, ones, preferred_element_type=F32)
            + jnp.dot(low, ones, preferred_element_type=F32)
        ) * (1.0 / 64)
        return (wide * lax.rsqrt(mean + EPS) * gain_).astype(BF)

    def iotas(rows_, cols_):
        return [lax.broadcasted_iota(jnp.int32, (rows_, cols_), i) for i in range(2)]

    r64, c64 = iotas(64, 64)
    kgain = jnp.sum(jnp.where(r64 == c64, kg[...], 0.0), axis=1, keepdims=True)
    r256, c256 = iotas(256, 256)
    ones256 = (r256 // 64 == c256 // 64).astype(BF)

    def key_norm(lo, n):
        wide = KX[:, lo:lo + n].astype(F32)
        mean = jnp.mean(wide * wide, axis=0, keepdims=True)
        KN[:, lo:lo + n] = (wide * lax.rsqrt(mean + EPS) * kgain).astype(BF)

    key_norm(128, 512)
    loads[5].wait()
    qgain = jnp.concatenate([qg[...]] * 4, axis=1)
    heads = [
        jnp.exp2(jnp.full((1, 1), (tp * 4 + h + 1).astype(F32) * -0.25)) for h in range(4)
    ]
    row = lax.broadcasted_iota(jnp.int32, (128, 128), 0)
    col = lax.broadcasted_iota(jnp.int32, (128, 128), 1)
    span = jnp.abs(
        lax.broadcasted_iota(jnp.int32, (128, 384), 1) - 128
        - lax.broadcasted_iota(jnp.int32, (128, 384), 0)
    ).astype(F32)

    def attend(b):
        qn = head_norm(QX[128 * b:128 * b + 128], qgain, ones256)
        kb, vb = KN[:, 128 * b:128 * b + 384], VX[:, 128 * b:128 * b + 384]
        docs = [DX[b + i].astype(F32) for i in range(3)]
        mine = jnp.transpose(jnp.broadcast_to(docs[1], (128, 128)))
        if b == 0:
            docs[0] = jnp.where(sp == 0, -1.0, docs[0])
        if b == 3:
            docs[2] = jnp.where(sp == Z * Y - 1, -1.0, docs[2])
        allowed = jnp.concatenate(
            [(mine == docs[0]) & (col >= row), mine == docs[1], (mine == docs[2]) & (col <= row)],
            axis=1,
        )
        outs = []
        for h in range(4):
            score = jnp.dot(qn[:, 64 * h:64 * h + 64], kb, preferred_element_type=F32)
            score = score * 0.125 - heads[h] * span
            score = jnp.where(allowed, score, -1e30)
            top = jnp.maximum(jnp.max(score, axis=1, keepdims=True), sink[h])
            p = jnp.exp(score - top)
            denom = jnp.sum(p, axis=1, keepdims=True) + jnp.exp(sink[h] - top)
            mixed = lax.dot_general(
                p.astype(BF), vb, (((1,), (1,)), ((), ())), preferred_element_type=F32
            )
            outs.append((mixed / denom).astype(BF))
        ATT[128 * b:128 * b + 128] = jnp.concatenate(outs, axis=1)

    def project(k):
        a = ATT[...].reshape(8, 2, 32, 256)[:, k].reshape(256, 256)
        p = jnp.dot(a, WO[...], preferred_element_type=F32).astype(BF)
        for side in range(2):
            PB1[k, :, side] = p[:, side * 1024:side * 1024 + 1024].reshape(8, 32, 1024)
        one.to_partner(k)

    def normalise(k):
        lo = 32 * k
        both = one.total(k)
        mid = (RES[lo:lo + 32].astype(F32) + jnp.concatenate(both, axis=1)).astype(BF).astype(F32)
        MID[lo:lo + 32] = mid
        scale = lax.rsqrt(jnp.mean(mid * mid, axis=-1, keepdims=True) + EPS)
        NALL[x * C + c, lo:lo + 32] = (mid * scale * gain[...]).astype(BF)
        rows.own(k)

    def up(n):
        lhs = NALL[...].reshape(512, 2048)
        rhs = WU[:, :, :, n * 512:n * 512 + 512].reshape(2048, 512)
        r = jnp.maximum(jnp.dot(lhs, rhs, preferred_element_type=F32), 0.0)
        ACT[:, n * 512:n * 512 + 512] = (r * r).astype(BF)

    def s_down(k):
        w = jnp.concatenate([WD[block_of(k, side)].reshape(256, 1024) for side in range(2)], axis=0)
        p = lax.dot_general(
            ACT[...], w, (((1,), (1,)), ((), ())), preferred_element_type=F32
        ).astype(BF)
        for side in range(2):
            PB2[k, :, side] = p[:, side * 256:side * 256 + 256].reshape(8, 64, 256)
        two.to_partner(k)

    def s_total(k):
        for side, part in enumerate(two.total(k)):
            cols = out_cols(k, side)
            OWN[:, cols] = (MID[:, cols] + part).astype(BF)
            keep.append(
                pltpu.make_async_copy(OWN.at[:, cols], out.at[x * C + c, :, cols], loc.at[8 + 2 * k + side])
            )
            keep[-1].start()
        done.own(k)

    keep = []
    def halo_block(side, lo, b):
        halo_got(side)
        key_norm(lo, 128)
        attend(b)

    for f, *args in (
        (attend, 1), (attend, 2), (ring_step, (0, 1), 1), (halo_block, 0, 0, 0),
        (halo_block, 1, 640, 3), (loads[6].wait,), (loads[7].wait,), (project, 0), (project, 1),
        (ring_step, (0, 1), 2), (pump, (0, 1), 0, 3), (one.far, 0), (chain, 1),
        (loop_step, 0, 1), (one.far, 1), (ring_step, (0, 1), 3), (pump, (0, 1), 3, 5),
        (pump, (0, 1), 8, 9), (one.grow, 0), (pump, (0, 1), 9, 11), (one.grow, 1),
        (ring_step, (0, 1), 4), (pump, (0, 1), 5, 7), (pump, (0, 1), 11, 12), (normalise, 0),
        (pump, (0, 1), 12, 13), (pump, (0, 1), 16, 17), (normalise, 1), (pump, (0, 1), 17, 18),
        (chain, 2), (loop_step, 0, 2), (pump, (0, 1), 18, 19), (pump, (0, 1), 7, 8),
        (rows.forward, 0), (pump, (0, 1), 13, 15), (rows.forward2, 0), (pump, (0, 1), 19, 21),
        (rows.forward, 1), (chain, 3), (loop_step, 0, 3), (rows.forward2, 1),
        (pump, (0, 1), 15, 16), (pump, (0, 1), 21, 22), (rows.last, 0), (pump, (0, 1), 22, 23),
        (pump, (0, 1), 24, 25), (loop_send, 1, 1), (down_send, 1, 1, 2), (rows.last, 1),
        (rows.finish, 0), (chain, 4), (loop_step, 0, 4), (pump, (0, 1), 23, 24),
        (loop_send, 2, 1), (loop_send, 3, 1), (down_send, 1, 2, 8), (rows.finish, 1),
        (pump, (0, 1), 25, 27), (loop_step, 1, 1), (pass_on, 1, 2), (pump, (0, 1), 27, 28),
        (up, 0), (up, 1), (loop_step, 2, 1), (pass_on, 2, 3), (loop_step, 3, 1), (pass_on, 3, 4),
        (loop_step, 1, 2), (pass_on, 4, 6), (loop_step, 2, 2), (pass_on, 6, 7),
        (loop_step, 3, 2), (pass_on, 7, 8), (s_down, 0), (loop_step, 1, 3), (take, 1, 2),
        (loop_step, 2, 3), (two.far, 0), (take, 2, 3), (loop_step, 3, 3), (loop_step, 1, 4),
        (s_down, 1), (loop_step, 2, 4), (take, 3, 4), (two.grow, 0), (loop_step, 3, 4),
        (s_down, 2), (two.far, 1), (take, 4, 6), (s_total, 0), (two.far, 2), (take, 6, 7),
        (two.grow, 1), (take, 7, 8), (s_down, 3), (done.forward, 0), (done.forward2, 0),
        (two.grow, 2), (two.far, 3), (s_total, 1), (done.last, 0), (s_total, 2),
        (done.finish, 0), (two.grow, 3), (done.forward, 1), (done.forward2, 1),
        (done.forward, 2), (done.forward2, 2), (s_total, 3), (done.last, 1), (done.last, 2),
        (done.finish, 1), (done.forward, 3), (done.finish, 2), (done.forward2, 3),
        (done.last, 3), (done.finish, 3),
    ):
        f(*args)
    for copy in keep:
        copy.wait()

    for i, ref in enumerate((
        WU.at[0, pl.ds(0, 7)], WU.at[pl.ds(0, 7)], WD.at[pl.ds(0, 7), pl.ds(0, 4)],
        WD.at[pl.ds(0, 7), pl.ds(0, 5)], RB1, SND1, RB2, SND2, NALL.at[pl.ds(0, 7)],
        NALL.at[pl.ds(0, 7)], KX.at[:, pl.ds(0, 256)], VX.at[:, pl.ds(0, 256)],
        DX.at[pl.ds(0, 2)],
    )):
        rc(ref, ref, left.at[i], hr.at[0, 0], partner).wait_send()


def shards(
    resid, queries, keys, values, documents, q_gain, k_gain, sink, w_out, n_gain, w_up, w_down
):
    rows, width = resid.shape
    vm, sm = pl.BlockSpec(memory_space=pltpu.VMEM), pl.BlockSpec(memory_space=pltpu.SMEM)
    hbm = pl.BlockSpec(memory_space=pltpu.HBM)
    H2 = 2048 // (2 * NC2)
    dma = pltpu.SemaphoreType.DMA
    out = pl.pallas_call(
        fused,
        out_shape=jax.ShapeDtypeStruct((8, rows // 8, width), BF),
        in_specs=[hbm, hbm, hbm, hbm, vm, vm, sm, hbm, hbm, vm, hbm, hbm],
        out_specs=pl.BlockSpec(memory_space=pl.ANY),
        scratch_shapes=[
            pltpu.VMEM((512, 256), BF),
            pltpu.VMEM((64, 768), BF),
            pltpu.VMEM((64, 768), BF),
            pltpu.VMEM((6, 1, 128), jnp.int32),
            pltpu.VMEM((64, 768), BF),
            pltpu.VMEM((512, 256), BF),
            pltpu.VMEM((8, 8, 32, 1024), BF),
            pltpu.VMEM((8, 8, 32, 1024), BF),
            pltpu.VMEM((256, 2048), BF),
            pltpu.VMEM((64, 2048), BF),
            pltpu.VMEM((NC1, 8, 2, 32, 1024), BF),
            pltpu.VMEM((NC1, 4, 2, 32, 1024), BF),
            pltpu.VMEM((NC1, 6, 32, 1024), BF),
            pltpu.VMEM((NC1, 6, 32, 1024), BF),
            pltpu.VMEM((NC2, 8, 2, 64, H2), BF),
            pltpu.VMEM((NC2, 4, 2, 64, H2), BF),
            pltpu.VMEM((NC2, 6, 64, H2), BF),
            pltpu.VMEM((NC2, 6, 64, H2), BF),
            pltpu.VMEM((8, 64, 2048), BF),
            pltpu.VMEM((64, 2048), F32),
            pltpu.VMEM((512, 1024), BF),
            pltpu.VMEM((64, 2048), BF),
            dma((16,)), dma((13,)), dma((2, 3)),
            dma((2, 2, 28)), dma((2, 2, 4)), dma((2, 18)), dma((4, 2, 4)),
            dma((NC1, 4)), dma((NC1, 6)), dma((NC2, 4)), dma((NC2, 6)),
            dma((NC1, 14)), dma((NC2, 14)),
        ],
        compiler_params=pltpu.CompilerParams(
            collective_id=0, has_side_effects=True, vmem_limit_bytes=56 * 1024 * 1024
        ),
        name="layer",
    )(
        queries, keys.T, values.T, documents.reshape(4, 1, 128), q_gain.reshape(1, -1),
        k_gain.reshape(1, -1), sink, w_out, resid, n_gain.reshape(1, -1), w_up, w_down.T,
    )
    return out.reshape(rows, width)


def solution(mesh):
    placed = (
        P("sp", None), P("sp", "tp"), P("sp", "tp"), P("sp", "tp"), P("sp"), P(), P(),
        P("tp"), P("tp", None), P(), P("sp", "tp"), P("tp", "sp"),
    )
    return jax.shard_map(
        shards, mesh=mesh, in_specs=placed, out_specs=P("sp", None), check_vma=False
    )
```

```python
import functools

import jax
import jax.numpy as jnp
from jax import lax
from jax.experimental import pallas as pl
from jax.experimental.pallas import tpu as pltpu
from jax.sharding import PartitionSpec as P

EPS = 1e-06
Z, Y, X, C = 8, 8, 4, 2
MESH = pl.DeviceIdType.MESH
BF, F32 = jnp.bfloat16, jnp.float32
NC1, NC2 = 2, 4


def fused(
    q_h, k_h, v_h, doc_h, qg_h, kg_h, sink_h, wout_h, resid_h, gain_h, wup_h, wdt_h, out,
    qg, kg, sink, gain, QX, KX, VX, DX, KN, ATT, WU, WD, WO, RES, PB1, RB1, SND1, RCV1, PB2, RB2, SND2, RCV2, NALL, MID, ACT, OWN,
    loc, left, hr, gr, rr, fr, er, d1r, n1r, d2r, n2r, a1r, a2r,
):
    sp, tp = lax.axis_index("sp"), lax.axis_index("tp")
    z, y = sp // Y, sp % Y
    x, c = tp // C, tp % C
    co = 1 - c

    def at_z(s):
        return (((z + s + Z) % Z) * Y + y, tp)

    def at_y(s):
        return (z * Y + (y + s + Y) % Y, tp)

    def xm(s):
        return (x + s + X) % X

    def at_x(s):
        return (sp, xm(s) * C + c)

    partner = (sp, x * C + co)

    def rc(src, dst, ss, rs, dev):
        return pltpu.make_async_remote_copy(
            src_ref=src, dst_ref=dst, send_sem=ss, recv_sem=rs, device_id=dev, device_id_type=MESH
        )

    def put(src, dst, ss, rs, dev):
        rc(src, dst, ss, rs, dev).start()

    def got(ref, rs):
        rc(ref, ref, left.at[0], rs, partner).wait_recv()

    loads = [
        pltpu.make_async_copy(wup_h, WU.at[z, y], loc.at[0]),
        pltpu.make_async_copy(k_h, KX.at[:, pl.ds(128, 512)], loc.at[1]),
        pltpu.make_async_copy(v_h, VX.at[:, pl.ds(128, 512)], loc.at[2]),
        pltpu.make_async_copy(doc_h, DX.at[pl.ds(1, 4)], loc.at[3]),
        pltpu.make_async_copy(wdt_h, WD.at[z, y], loc.at[4]),
        pltpu.make_async_copy(q_h, QX, loc.at[5]),
        pltpu.make_async_copy(wout_h, WO, loc.at[6]),
        pltpu.make_async_copy(
            resid_h.at[pl.ds(pl.multiple_of(tp * 64, 64), 64)], RES, loc.at[7]
        ),
    ]
    small = [
        pltpu.make_async_copy(src, dst, loc.at[16 + i])
        for i, (src, dst) in enumerate(((qg_h, qg), (kg_h, kg), (sink_h, sink), (gain_h, gain)))
    ]
    for copy in loads[:5] + small + loads[5:]:
        copy.start()
    barrier = pltpu.get_barrier_semaphore()
    after, before = ((sp + 1) % (Z * Y), tp), ((sp + Z * Y - 1) % (Z * Y), tp)
    near = [at_z(1), at_z(-1), at_y(1), at_y(-1), at_x(1), at_x(-1), at_x(2), partner, after, before]
    for dev in near:
        pl.semaphore_signal(barrier, inc=1, device_id=dev, device_id_type=MESH)
    pl.semaphore_wait(barrier, len(near))

    pieces = ((WU, 0, 512, "z"), (WU, 512, 512, "y"))
    ways = ((0, 1), (1, -1))

    def shard_ref(p, e, major, minor, half):
        buf, lo, n, axis = pieces[p]
        zz, yy = ((z + minor + 16) % 8, (y + major + 16) % 8)
        if axis == "y":
            zz, yy = ((z + major + 16) % 8, (y + minor + 16) % 8)
        rows_ = pl.ds(16 * e, 16) if half else slice(None)
        return buf.at[zz, yy, rows_, pl.ds(lo, n)]

    def ring_send(p, d):
        for e, s in ways:
            src = shard_ref(p, e, 0, -s * (d - 1), d == 4)
            dev = at_z(s) if pieces[p][3] == "z" else at_y(s)
            put(src, src, left.at[0], rr.at[d - 1], dev)

    def minor_off(j):
        return jnp.where(j % 2 == 1, -((j + 1) // 2), j // 2)

    def row_copy(p, e, s, d, j, m):
        src = shard_ref(p, e, -s * (d - 1), minor_off(j), False)
        dev = at_y(s) if pieces[p][3] == "z" else at_z(s)
        return rc(src, src, left.at[1], gr.at[m], dev)

    def row_send(p, j):
        for e, s in ways:
            row_copy(p, e, s, 1, j, j).start()

    def ring_step(d):
        got(WU.at[0, 0] if d == 4 else WU.at[0, pl.ds(0, 2)], rr.at[d - 1])
        if d < 4:
            for p in (0, 1):
                ring_send(p, d + 1)
        for j in (2 * d - 1, 2 * d):
            if j < 8:
                for p in (0, 1):
                    row_send(p, j)

    def pump(lo, hi):
        def step(m, _, to):
            d, j = m // 8 + 1, m % 8
            got(WU.at[0, pl.ds(0, 2)], gr.at[m])
            for p in (0, 1):
                for e, s in ways:
                    if to == (0, 1):
                        row_copy(p, e, s, d + 1, j, m + 8).start()
                    elif e in to:
                        row_copy(p, e, s, 4, m - 16, m + 8 - 4 * e).start()
            return 0

        for a, b, to in ((0, 16, (0, 1)), (16, 20, (0,)), (20, 24, (1,)), (24, 28, ())):
            a, b = max(a, lo), min(b, hi)
            if b - a == 1:
                step(a, 0, to)
            elif a < b:
                lax.fori_loop(a, b, functools.partial(step, to=to), 0)

    ring_base = (0, -3, 3, 4)

    def down_ref(e, dz, dy, half):
        ref = WD.at[(z + dz + 16) % 8, (y + dy + 16) % 8]
        return ref.at[pl.ds(16 * e, 16)] if half else ref

    def loop_send(r, d):
        for e, s in ways:
            src = down_ref(e, ring_base[r], -s * (d - 1), d == 4)
            put(src, src, left.at[2], er.at[r, d - 1], at_y(s))

    def loop_step(r, d):
        got(WD.at[0, 0] if d == 4 else WD.at[0, pl.ds(0, 2)], er.at[r, d - 1])
        if d < 4:
            loop_send(r, d + 1)

    def down_copy(e, s, d, j):
        m = 17 if d == 4 else (d - 1) * 8 + j
        src = down_ref(e, -s * (d - 1), minor_off(j), d == 4)
        return rc(src, src, left.at[3], fr.at[m], at_z(s))

    def down_send(d, lo, hi):
        for j in range(lo, hi):
            for e, s in ways:
                down_copy(e, s, d, j).start()

    def down_got(d, j):
        m = 17 if d == 4 else (d - 1) * 8 + j
        got(WD.at[0, 0] if d == 4 else WD.at[0, pl.ds(0, 2)], fr.at[m])

    def chain(d):
        down_got(d, 0)
        if d < 4:
            down_send(d + 1, 0, 1)

    def pass_on(lo, hi):
        def one_row(j, _):
            down_got(1, j)
            for e, s in ways:
                down_copy(e, s, 2, j).start()
            return 0

        lax.fori_loop(lo, hi, one_row, 0)

    def take(lo, hi):
        def one_row(j, _):
            down_got(2, j)
            return 0

        lax.fori_loop(lo, hi, one_row, 0)

    class Exchange:
        def __init__(self, PB, RB, SND, RCV, ds, dr, ns, nr):
            self.PB, self.RB, self.SND, self.RCV = PB, RB, SND, RCV
            self.ds, self.dr, self.ns, self.nr = ds, dr, ns, nr

        def to_partner(self, k):
            for q in (2, 1, 3, 0):
                b = xm(q)
                put(self.PB.at[k, b * C + co], self.RB.at[k, b], self.ds, self.dr.at[k, q],
                    partner)

        def pair(self, k, q, side):
            b = xm(q)
            return self.PB[k, b * C + c, side].astype(F32) + self.RB[k, b, side].astype(F32)

        def partner_got(self, k, q):
            got(self.RB.at[k, xm(q)], self.dr.at[k, q])

        def send(self, k, slot, value, dirn):
            self.SND[k, slot] = value.astype(BF)
            put(self.SND.at[k, slot], self.RCV.at[k, slot], self.ns, self.nr.at[k, slot],
                at_x(dirn))

        def have(self, k, slot):
            got(self.RCV.at[k, slot], self.nr.at[k, slot])
            return self.RCV[k, slot].astype(F32)

        def far(self, k):
            self.partner_got(k, 2)
            straight = self is two and k in direct
            self.send(k, 0, self.pair(k, 2, 0), 2 if straight else 1)
            self.send(k, 1, self.pair(k, 2, 1), 2 if straight else -1)
            self.partner_got(k, 1)
            self.send(k, 2, self.pair(k, 1, 1), 1)
            self.partner_got(k, 3)
            self.send(k, 3, self.pair(k, 3, 0), -1)
            if straight:
                self.send(k, 4, self.pair(k, 1, 0), 1)
                self.send(k, 5, self.pair(k, 3, 1), -1)

        def grow(self, k):
            self.send(k, 4, self.pair(k, 1, 0) + self.have(k, 0), 1)
            self.send(k, 5, self.pair(k, 3, 1) + self.have(k, 1), -1)

        def total(self, k):
            self.partner_got(k, 0)
            left = self.pair(k, 0, 0) + self.have(k, 3) + self.have(k, 4)
            right = self.pair(k, 0, 1) + self.have(k, 2) + self.have(k, 5)
            if self is two and k in direct:
                left, right = left + self.have(k, 0), right + self.have(k, 1)
            return left, right

    class Gather:
        def __init__(self, G, part, mine, s, r, size, direct=()):
            self.G, self.part, self.mine, self.s, self.r = G, part, mine, s, r
            self.size, self.direct = size, direct

        def ref(self, k, q, side, core):
            return self.G.at[(xm(q) * C + core, *self.part(k, side))]

        def go(self, k, slot, q, side, dev):
            ref = self.ref(k, q, side, c)
            src = self.mine.at[self.part(k, side)] if q == 0 else ref
            put(src, ref, self.s, self.r.at[k, min(slot, 6)], dev)

        def wait(self, k, slot, q, side, core):
            got(self.ref(k, q, side, core), self.r.at[k, slot])

        def own(self, k):
            self.go(k, 0, 0, 0, at_x(1))
            self.go(k, 1, 0, 1, at_x(-1))
            self.go(k, 2, 0, 1, at_x(1))
            self.go(k, 3, 0, 0, at_x(-1))
            if k in self.direct:
                self.go(k, 4, 0, 0, at_x(2))
                self.go(k, 5, 0, 1, at_x(2))
            self.go(k, 6, 0, 0, partner)
            self.go(k, 7, 0, 1, partner)

        def forward(self, k):
            self.wait(k, 0, 3, 0, c)
            if k not in self.direct:
                self.go(k, 4, 3, 0, at_x(1))
            self.wait(k, 1, 1, 1, c)
            if k not in self.direct:
                self.go(k, 5, 1, 1, at_x(-1))
            self.go(k, 8, 3, 0, partner)
            self.go(k, 9, 1, 1, partner)

        def forward2(self, k):
            self.wait(k, 2, 3, 1, c)
            self.go(k, 10, 3, 1, partner)
            self.wait(k, 3, 1, 0, c)
            self.go(k, 11, 1, 0, partner)

        def last(self, k):
            self.wait(k, 4, 2, 0, c)
            self.go(k, 12, 2, 0, partner)
            self.wait(k, 5, 2, 1, c)
            self.go(k, 13, 2, 1, partner)

        def finish(self, k):
            got(NALL.at[0] if self.size == 8 else NALL.at[pl.ds(0, 2)], self.r.at[k, 6])

    one = Exchange(PB1, RB1, SND1, RCV1, left.at[4], d1r, left.at[5], n1r)
    two = Exchange(PB2, RB2, SND2, RCV2, left.at[6], d2r, left.at[7], n2r)
    rows = Gather(
        NALL, lambda k, side: (pl.ds(32 * k, 32), pl.ds(side * 1024, 1024)), NALL.at[x * C + c],
        left.at[8], a1r, 16,
    )
    pairs = ((0, -1), (1, -3), (3, 4), (2, -2))

    def block_of(k, side):
        return (z + pairs[k][side] + 8) % 8

    def out_cols(k, side):
        return pl.ds(pl.multiple_of(block_of(k, side) * 256, 256), 256)

    direct = ()
    done = Gather(out, lambda k, side: (slice(None), out_cols(k, side)), OWN, left.at[9], a2r, 8, direct)

    loads[0].wait()
    ring_send(0, 1)
    ring_send(1, 1)
    for copy in loads[1:4]:
        copy.wait()
    halo = []
    for i, ref in enumerate((KX, VX, DX)):
        part = [
            ref.at[pl.ds(n, 1)] if i == 2 else ref.at[:, pl.ds(128 * n, 128)] for n in range(6)
        ]
        put(part[4], part[0], left.at[10 + i], hr.at[0, i], after)
        put(part[1], part[5], left.at[10 + i], hr.at[1, i], before)
        halo.append((part[0], part[5]))

    row_send(0, 0)
    row_send(1, 0)

    def halo_got(side):
        for i in range(3):
            got(halo[i][side], hr.at[side, i])

    loads[4].wait()
    loop_send(0, 1)
    down_send(1, 0, 1)

    def head_norm(rows_, gain_, ones):
        wide = rows_.astype(F32)
        square = wide * wide
        high = square.astype(BF)
        low = (square - high.astype(F32)).astype(BF)
        mean = (
            jnp.dot(high, ones, preferred_element_type=F32)
            + jnp.dot(low, ones, preferred_element_type=F32)
        ) * (1.0 / 64)
        return (wide * lax.rsqrt(mean + EPS) * gain_).astype(BF)

    def iotas(rows_, cols_):
        return [lax.broadcasted_iota(jnp.int32, (rows_, cols_), i) for i in range(2)]

    for copy in small:
        copy.wait()
    r64, c64 = iotas(64, 64)
    kgain = jnp.sum(jnp.where(r64 == c64, kg[...], 0.0), axis=1, keepdims=True)
    r256, c256 = iotas(256, 256)
    ones256 = (r256 // 64 == c256 // 64).astype(BF)

    def key_norm(lo, n):
        wide = KX[:, lo:lo + n].astype(F32)
        mean = jnp.mean(wide * wide, axis=0, keepdims=True)
        KN[:, lo:lo + n] = (wide * lax.rsqrt(mean + EPS) * kgain).astype(BF)

    key_norm(128, 512)
    loads[5].wait()
    qgain = jnp.concatenate([qg[...]] * 4, axis=1)
    heads = [
        jnp.exp2(jnp.full((1, 1), (tp * 4 + h + 1).astype(F32) * -0.25)) for h in range(4)
    ]
    row = lax.broadcasted_iota(jnp.int32, (128, 128), 0)
    col = lax.broadcasted_iota(jnp.int32, (128, 128), 1)
    span = jnp.abs(
        lax.broadcasted_iota(jnp.int32, (128, 384), 1) - 128
        - lax.broadcasted_iota(jnp.int32, (128, 384), 0)
    ).astype(F32)

    def attend(b):
        qn = head_norm(QX[128 * b:128 * b + 128], qgain, ones256)
        kb, vb = KN[:, 128 * b:128 * b + 384], VX[:, 128 * b:128 * b + 384]
        docs = [DX[b + i].astype(F32) for i in range(3)]
        mine = jnp.transpose(jnp.broadcast_to(docs[1], (128, 128)))
        if b == 0:
            docs[0] = jnp.where(sp == 0, -1.0, docs[0])
        if b == 3:
            docs[2] = jnp.where(sp == Z * Y - 1, -1.0, docs[2])
        allowed = jnp.concatenate(
            [(mine == docs[0]) & (col >= row), mine == docs[1], (mine == docs[2]) & (col <= row)],
            axis=1,
        )
        outs = []
        for h in range(4):
            score = jnp.dot(qn[:, 64 * h:64 * h + 64], kb, preferred_element_type=F32)
            score = score * 0.125 - heads[h] * span
            score = jnp.where(allowed, score, -1e30)
            top = jnp.maximum(jnp.max(score, axis=1, keepdims=True), sink[h])
            p = jnp.exp(score - top)
            denom = jnp.sum(p, axis=1, keepdims=True) + jnp.exp(sink[h] - top)
            mixed = lax.dot_general(
                p.astype(BF), vb, (((1,), (1,)), ((), ())), preferred_element_type=F32
            )
            outs.append((mixed / denom).astype(BF))
        ATT[128 * b:128 * b + 128] = jnp.concatenate(outs, axis=1)

    def project(k):
        a = ATT[...].reshape(8, 2, 32, 256)[:, k].reshape(256, 256)
        p = jnp.dot(a, WO[...], preferred_element_type=F32).astype(BF)
        for side in range(2):
            PB1[k, :, side] = p[:, side * 1024:side * 1024 + 1024].reshape(8, 32, 1024)
        one.to_partner(k)

    def normalise(k):
        lo = 32 * k
        both = one.total(k)
        mid = (RES[lo:lo + 32].astype(F32) + jnp.concatenate(both, axis=1)).astype(BF).astype(F32)
        MID[lo:lo + 32] = mid
        scale = lax.rsqrt(jnp.mean(mid * mid, axis=-1, keepdims=True) + EPS)
        NALL[x * C + c, lo:lo + 32] = (mid * scale * gain[...]).astype(BF)
        rows.own(k)

    def up(n):
        lhs = NALL[...].reshape(512, 2048)
        rhs = WU[:, :, :, n * 512:n * 512 + 512].reshape(2048, 512)
        r = jnp.maximum(jnp.dot(lhs, rhs, preferred_element_type=F32), 0.0)
        ACT[:, n * 512:n * 512 + 512] = (r * r).astype(BF)

    def s_down(k):
        w = jnp.concatenate([WD[block_of(k, side)].reshape(256, 1024) for side in range(2)], axis=0)
        p = lax.dot_general(
            ACT[...], w, (((1,), (1,)), ((), ())), preferred_element_type=F32
        ).astype(BF)
        for side in range(2):
            PB2[k, :, side] = p[:, side * 256:side * 256 + 256].reshape(8, 64, 256)
        two.to_partner(k)

    def s_total(k):
        for side, part in enumerate(two.total(k)):
            cols = out_cols(k, side)
            OWN[:, cols] = (MID[:, cols] + part).astype(BF)
            keep.append(
                pltpu.make_async_copy(OWN.at[:, cols], out.at[x * C + c, :, cols], loc.at[8 + 2 * k + side])
            )
            keep[-1].start()
        done.own(k)

    keep = []
    def halo_block(side, lo, b):
        halo_got(side)
        key_norm(lo, 128)
        attend(b)

    for f, *args in (
        (attend, 1), (attend, 2), (ring_step, 1), (halo_block, 0, 0, 0), (pump, 0, 1),
        (chain, 1), (halo_block, 1, 640, 3), (ring_step, 2), (loop_step, 0, 1), (loads[6].wait,),
        (loads[7].wait,), (project, 0), (project, 1), (pump, 1, 3), (pump, 8, 9), (one.far, 0),
        (one.far, 1), (chain, 2), (ring_step, 3), (pump, 3, 5), (loop_step, 0, 2), (one.grow, 0),
        (pump, 9, 11), (pump, 16, 17), (chain, 3), (ring_step, 4), (one.grow, 1), (pump, 5, 7),
        (pump, 11, 13), (normalise, 0), (loop_step, 0, 3), (normalise, 1), (pump, 17, 18),
        (chain, 4), (pump, 18, 19), (down_send, 1, 1, 2), (pump, 7, 8), (pump, 13, 14),
        (rows.forward, 0), (pump, 14, 15), (pump, 19, 20), (loop_send, 1, 1), (rows.forward2, 0),
        (pump, 20, 21), (loop_step, 0, 4), (down_send, 1, 2, 3), (rows.forward, 1),
        (pump, 15, 16), (pump, 21, 22), (rows.forward2, 1), (pump, 22, 23), (loop_send, 2, 1),
        (rows.last, 0), (down_send, 1, 3, 4), (pump, 24, 25), (loop_send, 3, 1), (rows.last, 1),
        (down_send, 1, 4, 5), (pump, 23, 24), (loop_step, 1, 1), (down_send, 1, 5, 8),
        (pass_on, 1, 3), (pump, 25, 27), (loop_step, 2, 1), (pass_on, 3, 4), (loop_step, 3, 1),
        (pass_on, 4, 5), (pump, 27, 28), (rows.finish, 0), (rows.finish, 1), (up, 0),
        (loop_step, 1, 2), (up, 1), (loop_step, 2, 2), (pass_on, 5, 7), (loop_step, 3, 2),
        (pass_on, 7, 8), (s_down, 0), (loop_step, 1, 3), (take, 1, 2), (two.far, 0),
        (loop_step, 2, 3), (take, 2, 3), (loop_step, 3, 3), (take, 3, 4), (loop_step, 1, 4),
        (s_down, 1), (two.grow, 0), (take, 4, 5), (loop_step, 2, 4), (two.far, 1), (take, 5, 6),
        (loop_step, 3, 4), (s_down, 2), (take, 6, 7), (s_total, 0), (two.far, 2), (take, 7, 8),
        (s_down, 3), (two.grow, 1), (two.far, 3), (done.forward, 0), (done.forward2, 0),
        (two.grow, 2), (s_total, 1), (two.grow, 3), (done.last, 0), (s_total, 2),
        (done.forward, 1), (done.forward2, 1), (s_total, 3), (done.forward, 2),
        (done.forward2, 2), (done.last, 1), (done.forward, 3), (done.forward2, 3),
        (done.last, 2), (done.last, 3), (done.finish, 0), (done.finish, 1), (done.finish, 2),
        (done.finish, 3),
    ):
        f(*args)
    for copy in keep:
        copy.wait()

    for i, ref in enumerate((
        WU.at[0, pl.ds(0, 7)], WU.at[pl.ds(0, 7)], WD.at[pl.ds(0, 7), pl.ds(0, 4)],
        WD.at[pl.ds(0, 7), pl.ds(0, 5)], RB1, SND1, RB2, SND2, NALL.at[pl.ds(0, 7)],
        NALL.at[pl.ds(0, 7)], KX.at[:, pl.ds(0, 256)], VX.at[:, pl.ds(0, 256)],
        DX.at[pl.ds(0, 2)],
    )):
        rc(ref, ref, left.at[i], hr.at[0, 0], partner).wait_send()


def shards(
    resid, queries, keys, values, documents, q_gain, k_gain, sink, w_out, n_gain, w_up, w_down
):
    rows, width = resid.shape
    hbm = pl.BlockSpec(memory_space=pltpu.HBM)
    H2 = 2048 // (2 * NC2)
    dma = pltpu.SemaphoreType.DMA
    out = pl.pallas_call(
        fused,
        out_shape=jax.ShapeDtypeStruct((8, rows // 8, width), BF),
        in_specs=[hbm] * 12,
        out_specs=pl.BlockSpec(memory_space=pl.ANY),
        scratch_shapes=[
            pltpu.VMEM((1, 64), F32),
            pltpu.VMEM((1, 64), F32),
            pltpu.SMEM((4,), F32),
            pltpu.VMEM((1, 2048), F32),
            pltpu.VMEM((512, 256), BF),
            pltpu.VMEM((64, 768), BF),
            pltpu.VMEM((64, 768), BF),
            pltpu.VMEM((6, 1, 128), jnp.int32),
            pltpu.VMEM((64, 768), BF),
            pltpu.VMEM((512, 256), BF),
            pltpu.VMEM((8, 8, 32, 1024), BF),
            pltpu.VMEM((8, 8, 32, 1024), BF),
            pltpu.VMEM((256, 2048), BF),
            pltpu.VMEM((64, 2048), BF),
            pltpu.VMEM((NC1, 8, 2, 32, 1024), BF),
            pltpu.VMEM((NC1, 4, 2, 32, 1024), BF),
            pltpu.VMEM((NC1, 6, 32, 1024), BF),
            pltpu.VMEM((NC1, 6, 32, 1024), BF),
            pltpu.VMEM((NC2, 8, 2, 64, H2), BF),
            pltpu.VMEM((NC2, 4, 2, 64, H2), BF),
            pltpu.VMEM((NC2, 6, 64, H2), BF),
            pltpu.VMEM((NC2, 6, 64, H2), BF),
            pltpu.VMEM((8, 64, 2048), BF),
            pltpu.VMEM((64, 2048), F32),
            pltpu.VMEM((512, 1024), BF),
            pltpu.VMEM((64, 2048), BF),
            dma((20,)), dma((13,)), dma((2, 3)),
            dma((28,)), dma((4,)), dma((18,)), dma((4, 4)),
            dma((NC1, 4)), dma((NC1, 6)), dma((NC2, 4)), dma((NC2, 6)),
            dma((NC1, 7)), dma((NC2, 7)),
        ],
        compiler_params=pltpu.CompilerParams(
            collective_id=0, has_side_effects=True, vmem_limit_bytes=56 * 1024 * 1024
        ),
        name="layer",
    )(
        queries, keys.T, values.T, documents.reshape(4, 1, 128), q_gain.reshape(1, -1),
        k_gain.reshape(1, -1), sink, w_out, resid, n_gain.reshape(1, -1), w_up, w_down.T,
    )
    return out.reshape(rows, width)


def solution(mesh):
    placed = (
        P("sp", None), P("sp", "tp"), P("sp", "tp"), P("sp", "tp"), P("sp"), P(), P(),
        P("tp"), P("tp", None), P(), P("sp", "tp"), P("tp", "sp"),
    )
    return jax.shard_map(
        shards, mesh=mesh, in_specs=placed, out_specs=P("sp", None), check_vma=False
    )
```

```python
import functools

import jax
import jax.numpy as jnp
from jax import lax
from jax.experimental import pallas as pl
from jax.experimental.pallas import tpu as pltpu
from jax.sharding import PartitionSpec as P

EPS = 1e-06
Z, Y, X, C = 8, 8, 4, 2
MESH = pl.DeviceIdType.MESH
BF, F32 = jnp.bfloat16, jnp.float32
NC1, NC2 = 2, 4


def fused(
    q_h, k_h, v_h, doc_h, qg_h, kg_h, sink_h, wout_h, resid_h, gain_h, wup_h, wdt_h, out,
    qg, kg, sink, gain, QX, KX, VX, DX, KN, ATT, WU, WD, WO, RES, PB1, RB1, SND1, RCV1, PB2, RB2, SND2, RCV2, NALL, MID, ACT, ALL,
    loc, left, hr, gr, rr, fr, er, d1r, n1r, d2r, n2r, a1r, a2r,
):
    sp, tp = lax.axis_index("sp"), lax.axis_index("tp")
    z, y = sp // Y, sp % Y
    x, c = tp // C, tp % C
    co = 1 - c

    def at_z(s):
        return (((z + s + Z) % Z) * Y + y, tp)

    def at_y(s):
        return (z * Y + (y + s + Y) % Y, tp)

    def xm(s):
        return (x + s + X) % X

    def at_x(s):
        return (sp, xm(s) * C + c)

    partner = (sp, x * C + co)

    def rc(src, dst, ss, rs, dev):
        return pltpu.make_async_remote_copy(
            src_ref=src, dst_ref=dst, send_sem=ss, recv_sem=rs, device_id=dev, device_id_type=MESH
        )

    def put(src, dst, ss, rs, dev):
        rc(src, dst, ss, rs, dev).start()

    def got(ref, rs):
        rc(ref, ref, left.at[0], rs, partner).wait_recv()

    loads = [
        pltpu.make_async_copy(wup_h, WU.at[z, y], loc.at[0]),
        pltpu.make_async_copy(k_h, KX.at[:, pl.ds(128, 512)], loc.at[1]),
        pltpu.make_async_copy(v_h, VX.at[:, pl.ds(128, 512)], loc.at[2]),
        pltpu.make_async_copy(doc_h, DX.at[pl.ds(1, 4)], loc.at[3]),
        pltpu.make_async_copy(wdt_h, WD.at[z, y], loc.at[4]),
        pltpu.make_async_copy(q_h, QX, loc.at[5]),
        pltpu.make_async_copy(wout_h, WO, loc.at[6]),
        pltpu.make_async_copy(
            resid_h.at[pl.ds(pl.multiple_of(tp * 64, 64), 64)], RES, loc.at[7]
        ),
    ]
    small = [
        pltpu.make_async_copy(src, dst, loc.at[16 + i])
        for i, (src, dst) in enumerate(((qg_h, qg), (kg_h, kg), (sink_h, sink), (gain_h, gain)))
    ]
    for copy in loads[:5] + small + loads[5:]:
        copy.start()
    barrier = pltpu.get_barrier_semaphore()
    after, before = ((sp + 1) % (Z * Y), tp), ((sp + Z * Y - 1) % (Z * Y), tp)
    near = [at_z(1), at_z(-1), at_y(1), at_y(-1), at_x(1), at_x(-1), at_x(2), partner, after, before]
    for dev in near:
        pl.semaphore_signal(barrier, inc=1, device_id=dev, device_id_type=MESH)
    pl.semaphore_wait(barrier, len(near))

    pieces = ((WU, 0, 512, "z"), (WU, 512, 512, "y"))
    ways = ((0, 1), (1, -1))

    def shard_ref(p, e, major, minor, half):
        buf, lo, n, axis = pieces[p]
        zz, yy = ((z + minor + 16) % 8, (y + major + 16) % 8)
        if axis == "y":
            zz, yy = ((z + major + 16) % 8, (y + minor + 16) % 8)
        rows_ = pl.ds(16 * e, 16) if half else slice(None)
        return buf.at[zz, yy, rows_, pl.ds(lo, n)]

    def ring_send(p, d):
        for e, s in ways:
            src = shard_ref(p, e, 0, -s * (d - 1), d == 4)
            dev = at_z(s) if pieces[p][3] == "z" else at_y(s)
            put(src, src, left.at[0], rr.at[d - 1], dev)

    def minor_off(j):
        return jnp.where(j % 2 == 1, -((j + 1) // 2), j // 2)

    def row_copy(p, e, s, d, j, m):
        src = shard_ref(p, e, -s * (d - 1), minor_off(j), False)
        dev = at_y(s) if pieces[p][3] == "z" else at_z(s)
        return rc(src, src, left.at[1], gr.at[m], dev)

    def row_send(p, j):
        for e, s in ways:
            row_copy(p, e, s, 1, j, j).start()

    def ring_step(d):
        got(WU.at[0, 0] if d == 4 else WU.at[0, pl.ds(0, 2)], rr.at[d - 1])
        if d < 4:
            for p in (0, 1):
                ring_send(p, d + 1)
        for j in (2 * d - 1, 2 * d):
            if j < 8:
                for p in (0, 1):
                    row_send(p, j)

    def pump(lo, hi):
        def step(m, _, to):
            d, j = m // 8 + 1, m % 8
            got(WU.at[0, pl.ds(0, 2)], gr.at[m])
            for p in (0, 1):
                for e, s in ways:
                    if to == (0, 1):
                        row_copy(p, e, s, d + 1, j, m + 8).start()
                    elif e in to:
                        row_copy(p, e, s, 4, m - 16, m + 8 - 4 * e).start()
            return 0

        for a, b, to in ((0, 16, (0, 1)), (16, 20, (0,)), (20, 24, (1,)), (24, 28, ())):
            a, b = max(a, lo), min(b, hi)
            if b - a == 1:
                step(a, 0, to)
            elif a < b:
                lax.fori_loop(a, b, functools.partial(step, to=to), 0)

    ring_base = (0, -3, 3, 4)

    def down_ref(e, dz, dy, half):
        ref = WD.at[(z + dz + 16) % 8, (y + dy + 16) % 8]
        return ref.at[pl.ds(16 * e, 16)] if half else ref

    def loop_send(r, d):
        for e, s in ways:
            src = down_ref(e, ring_base[r], -s * (d - 1), d == 4)
            put(src, src, left.at[2], er.at[r, d - 1], at_y(s))

    def loop_step(r, d):
        got(WD.at[0, 0] if d == 4 else WD.at[0, pl.ds(0, 2)], er.at[r, d - 1])
        if d < 4:
            loop_send(r, d + 1)

    def down_copy(e, s, d, j):
        m = 17 if d == 4 else (d - 1) * 8 + j
        src = down_ref(e, -s * (d - 1), minor_off(j), d == 4)
        return rc(src, src, left.at[3], fr.at[m], at_z(s))

    def down_send(d, lo, hi):
        for j in range(lo, hi):
            for e, s in ways:
                down_copy(e, s, d, j).start()

    def down_got(d, j):
        m = 17 if d == 4 else (d - 1) * 8 + j
        got(WD.at[0, 0] if d == 4 else WD.at[0, pl.ds(0, 2)], fr.at[m])

    def chain(d):
        down_got(d, 0)
        if d < 4:
            down_send(d + 1, 0, 1)

    def pass_on(lo, hi):
        def one_row(j, _):
            down_got(1, j)
            for e, s in ways:
                down_copy(e, s, 2, j).start()
            return 0

        lax.fori_loop(lo, hi, one_row, 0)

    def take(lo, hi):
        def one_row(j, _):
            down_got(2, j)
            return 0

        lax.fori_loop(lo, hi, one_row, 0)

    class Exchange:
        def __init__(self, PB, RB, SND, RCV, ds, dr, ns, nr):
            self.PB, self.RB, self.SND, self.RCV = PB, RB, SND, RCV
            self.ds, self.dr, self.ns, self.nr = ds, dr, ns, nr

        def to_partner(self, k):
            for q in (2, 1, 3, 0):
                b = xm(q)
                put(self.PB.at[k, b * C + co], self.RB.at[k, b], self.ds, self.dr.at[k, q],
                    partner)

        def pair(self, k, q, side):
            b = xm(q)
            return self.PB[k, b * C + c, side].astype(F32) + self.RB[k, b, side].astype(F32)

        def partner_got(self, k, q):
            got(self.RB.at[k, xm(q)], self.dr.at[k, q])

        def send(self, k, slot, value, dirn):
            self.SND[k, slot] = value.astype(BF)
            put(self.SND.at[k, slot], self.RCV.at[k, slot], self.ns, self.nr.at[k, slot],
                at_x(dirn))

        def have(self, k, slot):
            got(self.RCV.at[k, slot], self.nr.at[k, slot])
            return self.RCV[k, slot].astype(F32)

        def far(self, k):
            self.partner_got(k, 2)
            straight = self is two and k in direct
            self.send(k, 0, self.pair(k, 2, 0), 2 if straight else 1)
            self.send(k, 1, self.pair(k, 2, 1), 2 if straight else -1)
            self.partner_got(k, 1)
            self.send(k, 2, self.pair(k, 1, 1), 1)
            self.partner_got(k, 3)
            self.send(k, 3, self.pair(k, 3, 0), -1)
            if straight:
                self.send(k, 4, self.pair(k, 1, 0), 1)
                self.send(k, 5, self.pair(k, 3, 1), -1)

        def grow(self, k):
            self.send(k, 4, self.pair(k, 1, 0) + self.have(k, 0), 1)
            self.send(k, 5, self.pair(k, 3, 1) + self.have(k, 1), -1)

        def total(self, k):
            self.partner_got(k, 0)
            left = self.pair(k, 0, 0) + self.have(k, 3) + self.have(k, 4)
            right = self.pair(k, 0, 1) + self.have(k, 2) + self.have(k, 5)
            if self is two and k in direct:
                left, right = left + self.have(k, 0), right + self.have(k, 1)
            return left, right

    class Gather:
        def __init__(self, G, part, mine, s, r, size, direct=()):
            self.G, self.part, self.mine, self.s, self.r = G, part, mine, s, r
            self.size, self.direct = size, direct

        def ref(self, k, q, side, core):
            return self.G.at[(xm(q) * C + core, *self.part(k, side))]

        def go(self, k, slot, q, side, dev):
            ref = self.ref(k, q, side, c)
            src = self.mine.at[self.part(k, side)] if q == 0 else ref
            put(src, ref, self.s, self.r.at[k, min(slot, 6)], dev)

        def wait(self, k, slot, q, side, core):
            got(self.ref(k, q, side, core), self.r.at[k, slot])

        def own(self, k):
            self.go(k, 0, 0, 0, at_x(1))
            self.go(k, 1, 0, 1, at_x(-1))
            self.go(k, 2, 0, 1, at_x(1))
            self.go(k, 3, 0, 0, at_x(-1))
            if k in self.direct:
                self.go(k, 4, 0, 0, at_x(2))
                self.go(k, 5, 0, 1, at_x(2))
            self.go(k, 6, 0, 0, partner)
            self.go(k, 7, 0, 1, partner)

        def forward(self, k):
            self.wait(k, 0, 3, 0, c)
            if k not in self.direct:
                self.go(k, 4, 3, 0, at_x(1))
            self.wait(k, 1, 1, 1, c)
            if k not in self.direct:
                self.go(k, 5, 1, 1, at_x(-1))
            self.go(k, 8, 3, 0, partner)
            self.go(k, 9, 1, 1, partner)

        def forward2(self, k):
            self.wait(k, 2, 3, 1, c)
            self.go(k, 10, 3, 1, partner)
            self.wait(k, 3, 1, 0, c)
            self.go(k, 11, 1, 0, partner)

        def last(self, k):
            self.wait(k, 4, 2, 0, c)
            self.go(k, 12, 2, 0, partner)
            self.wait(k, 5, 2, 1, c)
            self.go(k, 13, 2, 1, partner)

        def finish(self, k):
            got(NALL.at[0] if self.size == 8 else NALL.at[pl.ds(0, 2)], self.r.at[k, 6])

    one = Exchange(PB1, RB1, SND1, RCV1, left.at[4], d1r, left.at[5], n1r)
    two = Exchange(PB2, RB2, SND2, RCV2, left.at[6], d2r, left.at[7], n2r)
    rows = Gather(
        NALL, lambda k, side: (pl.ds(32 * k, 32), pl.ds(side * 1024, 1024)), NALL.at[x * C + c],
        left.at[8], a1r, 16,
    )
    pairs = ((0, -1), (1, -3), (3, 4), (2, -2))

    def block_of(k, side):
        return (z + pairs[k][side] + 8) % 8

    def out_cols(k, side):
        return pl.ds(pl.multiple_of(block_of(k, side) * 256, 256), 256)

    direct = ()
    done = Gather(
        ALL, lambda k, side: (slice(None), out_cols(k, side)), ALL.at[x * C + c], left.at[9], a2r,
        8, direct,
    )

    loads[0].wait()
    ring_send(0, 1)
    ring_send(1, 1)
    for copy in loads[1:4]:
        copy.wait()
    halo = []
    for i, ref in enumerate((KX, VX, DX)):
        part = [
            ref.at[pl.ds(n, 1)] if i == 2 else ref.at[:, pl.ds(128 * n, 128)] for n in range(6)
        ]
        put(part[4], part[0], left.at[10 + i], hr.at[0, i], after)
        put(part[1], part[5], left.at[10 + i], hr.at[1, i], before)
        halo.append((part[0], part[5]))

    row_send(0, 0)
    row_send(1, 0)

    def halo_got(side):
        for i in range(3):
            got(halo[i][side], hr.at[side, i])

    loads[4].wait()
    loop_send(0, 1)
    down_send(1, 0, 1)

    def head_norm(rows_, gain_, ones):
        wide = rows_.astype(F32)
        square = wide * wide
        high = square.astype(BF)
        low = (square - high.astype(F32)).astype(BF)
        mean = (
            jnp.dot(high, ones, preferred_element_type=F32)
            + jnp.dot(low, ones, preferred_element_type=F32)
        ) * (1.0 / 64)
        return (wide * lax.rsqrt(mean + EPS) * gain_).astype(BF)

    def iotas(rows_, cols_):
        return [lax.broadcasted_iota(jnp.int32, (rows_, cols_), i) for i in range(2)]

    for copy in small:
        copy.wait()
    r64, c64 = iotas(64, 64)
    kgain = jnp.sum(jnp.where(r64 == c64, kg[...], 0.0), axis=1, keepdims=True)
    r256, c256 = iotas(256, 256)
    ones256 = (r256 // 64 == c256 // 64).astype(BF)

    def key_norm(lo, n):
        wide = KX[:, lo:lo + n].astype(F32)
        mean = jnp.mean(wide * wide, axis=0, keepdims=True)
        KN[:, lo:lo + n] = (wide * lax.rsqrt(mean + EPS) * kgain).astype(BF)

    key_norm(128, 512)
    loads[5].wait()
    qgain = jnp.concatenate([qg[...]] * 4, axis=1)
    heads = [
        jnp.exp2(jnp.full((1, 1), (tp * 4 + h + 1).astype(F32) * -0.25)) for h in range(4)
    ]
    row = lax.broadcasted_iota(jnp.int32, (128, 128), 0)
    col = lax.broadcasted_iota(jnp.int32, (128, 128), 1)
    span = jnp.abs(
        lax.broadcasted_iota(jnp.int32, (128, 384), 1) - 128
        - lax.broadcasted_iota(jnp.int32, (128, 384), 0)
    ).astype(F32)

    def attend(b):
        qn = head_norm(QX[128 * b:128 * b + 128], qgain, ones256)
        kb, vb = KN[:, 128 * b:128 * b + 384], VX[:, 128 * b:128 * b + 384]
        docs = [DX[b + i].astype(F32) for i in range(3)]
        mine = jnp.transpose(jnp.broadcast_to(docs[1], (128, 128)))
        if b == 0:
            docs[0] = jnp.where(sp == 0, -1.0, docs[0])
        if b == 3:
            docs[2] = jnp.where(sp == Z * Y - 1, -1.0, docs[2])
        allowed = jnp.concatenate(
            [(mine == docs[0]) & (col >= row), mine == docs[1], (mine == docs[2]) & (col <= row)],
            axis=1,
        )
        outs = []
        for h in range(4):
            score = jnp.dot(qn[:, 64 * h:64 * h + 64], kb, preferred_element_type=F32)
            score = score * 0.125 - heads[h] * span
            score = jnp.where(allowed, score, -1e30)
            top = jnp.maximum(jnp.max(score, axis=1, keepdims=True), sink[h])
            p = jnp.exp(score - top)
            denom = jnp.sum(p, axis=1, keepdims=True) + jnp.exp(sink[h] - top)
            mixed = lax.dot_general(
                p.astype(BF), vb, (((1,), (1,)), ((), ())), preferred_element_type=F32
            )
            outs.append((mixed / denom).astype(BF))
        ATT[128 * b:128 * b + 128] = jnp.concatenate(outs, axis=1)

    def project(k):
        a = ATT[...].reshape(8, 2, 32, 256)[:, k].reshape(256, 256)
        p = jnp.dot(a, WO[...], preferred_element_type=F32).astype(BF)
        for side in range(2):
            PB1[k, :, side] = p[:, side * 1024:side * 1024 + 1024].reshape(8, 32, 1024)
        one.to_partner(k)

    def normalise(k):
        lo = 32 * k
        both = one.total(k)
        mid = (RES[lo:lo + 32].astype(F32) + jnp.concatenate(both, axis=1)).astype(BF).astype(F32)
        MID[lo:lo + 32] = mid
        scale = lax.rsqrt(jnp.mean(mid * mid, axis=-1, keepdims=True) + EPS)
        NALL[x * C + c, lo:lo + 32] = (mid * scale * gain[...]).astype(BF)
        rows.own(k)

    def up(n):
        lhs = NALL[...].reshape(512, 2048)
        rhs = WU[:, :, :, n * 512:n * 512 + 512].reshape(2048, 512)
        r = jnp.maximum(jnp.dot(lhs, rhs, preferred_element_type=F32), 0.0)
        ACT[:, n * 512:n * 512 + 512] = (r * r).astype(BF)

    def s_down(k):
        w = jnp.concatenate([WD[block_of(k, side)].reshape(256, 1024) for side in range(2)], axis=0)
        p = lax.dot_general(
            ACT[...], w, (((1,), (1,)), ((), ())), preferred_element_type=F32
        ).astype(BF)
        for side in range(2):
            PB2[k, :, side] = p[:, side * 256:side * 256 + 256].reshape(8, 64, 256)
        two.to_partner(k)

    def s_total(k):
        for side, part in enumerate(two.total(k)):
            cols = out_cols(k, side)
            ALL[x * C + c, :, cols] = (MID[:, cols] + part).astype(BF)
        done.own(k)

    keep = []

    def hand_over(k):
        done.finish(k)
        for side in range(2):
            cols = out_cols(k, side)
            keep.append(
                pltpu.make_async_copy(
                    ALL.at[:, :, cols], out.at[:, :, cols], loc.at[8 + 2 * k + side]
                )
            )
            keep[-1].start()

    def halo_block(side, lo, b):
        halo_got(side)
        key_norm(lo, 128)
        attend(b)

    for f, *args in (
        (attend, 1), (ring_step, 1), (attend, 2), (pump, 0, 1), (halo_block, 0, 0, 0),
        (chain, 1), (halo_block, 1, 640, 3), (ring_step, 2), (loop_step, 0, 1), (loads[6].wait,),
        (loads[7].wait,), (project, 0), (project, 1), (pump, 1, 3), (pump, 8, 9), (one.far, 0),
        (one.far, 1), (chain, 2), (ring_step, 3), (pump, 3, 5), (loop_step, 0, 2), (one.grow, 0),
        (pump, 9, 11), (pump, 16, 17), (chain, 3), (ring_step, 4), (one.grow, 1), (pump, 5, 7),
        (pump, 11, 13), (normalise, 0), (loop_step, 0, 3), (normalise, 1), (pump, 17, 18),
        (chain, 4), (pump, 18, 19), (down_send, 1, 1, 2), (pump, 7, 8), (pump, 13, 14),
        (rows.forward, 0), (pump, 14, 15), (pump, 19, 20), (loop_send, 1, 1), (rows.forward2, 0),
        (pump, 20, 21), (loop_step, 0, 4), (down_send, 1, 2, 3), (rows.forward, 1),
        (pump, 15, 16), (pump, 21, 22), (rows.forward2, 1), (pump, 22, 23), (loop_send, 2, 1),
        (rows.last, 0), (down_send, 1, 3, 4), (pump, 24, 25), (loop_send, 3, 1), (rows.last, 1),
        (down_send, 1, 4, 5), (pump, 23, 24), (loop_step, 1, 1), (down_send, 1, 5, 8),
        (pass_on, 1, 3), (pump, 25, 27), (loop_step, 2, 1), (pass_on, 3, 4), (loop_step, 3, 1),
        (pass_on, 4, 5), (pump, 27, 28), (rows.finish, 0), (rows.finish, 1), (up, 0),
        (loop_step, 1, 2), (up, 1), (loop_step, 2, 2), (pass_on, 5, 7), (loop_step, 3, 2),
        (pass_on, 7, 8), (s_down, 0), (loop_step, 1, 3), (take, 1, 2), (two.far, 0),
        (loop_step, 2, 3), (take, 2, 3), (loop_step, 3, 3), (take, 3, 4), (loop_step, 1, 4),
        (s_down, 1), (two.grow, 0), (take, 4, 5), (loop_step, 2, 4), (two.far, 1), (take, 5, 6),
        (loop_step, 3, 4), (s_down, 2), (take, 6, 7), (s_total, 0), (two.far, 2), (take, 7, 8),
        (s_down, 3), (two.grow, 1), (two.far, 3), (done.forward, 0), (done.forward2, 0),
        (two.grow, 2), (s_total, 1), (two.grow, 3), (done.last, 0), (s_total, 2),
        (done.forward, 1), (done.forward2, 1), (s_total, 3), (done.forward, 2),
        (done.forward2, 2), (done.last, 1), (done.forward, 3), (done.forward2, 3),
        (hand_over, 0), (done.last, 2), (hand_over, 1), (done.last, 3), (hand_over, 2),
        (hand_over, 3),
    ):
        f(*args)
    for copy in keep:
        copy.wait()

    for i, ref in enumerate((
        WU.at[0, pl.ds(0, 7)], WU.at[pl.ds(0, 7)], WD.at[pl.ds(0, 7), pl.ds(0, 4)],
        WD.at[pl.ds(0, 7), pl.ds(0, 5)], RB1, SND1, RB2, SND2, NALL.at[pl.ds(0, 7)],
        NALL.at[pl.ds(0, 7)], KX.at[:, pl.ds(0, 256)], VX.at[:, pl.ds(0, 256)],
        DX.at[pl.ds(0, 2)],
    )):
        rc(ref, ref, left.at[i], hr.at[0, 0], partner).wait_send()


def shards(
    resid, queries, keys, values, documents, q_gain, k_gain, sink, w_out, n_gain, w_up, w_down
):
    rows, width = resid.shape
    hbm = pl.BlockSpec(memory_space=pltpu.HBM)
    H2 = 2048 // (2 * NC2)
    dma = pltpu.SemaphoreType.DMA
    out = pl.pallas_call(
        fused,
        out_shape=jax.ShapeDtypeStruct((8, rows // 8, width), BF),
        in_specs=[hbm] * 12,
        out_specs=pl.BlockSpec(memory_space=pl.ANY),
        scratch_shapes=[
            pltpu.VMEM((1, 64), F32),
            pltpu.VMEM((1, 64), F32),
            pltpu.SMEM((4,), F32),
            pltpu.VMEM((1, 2048), F32),
            pltpu.VMEM((512, 256), BF),
            pltpu.VMEM((64, 768), BF),
            pltpu.VMEM((64, 768), BF),
            pltpu.VMEM((6, 1, 128), jnp.int32),
            pltpu.VMEM((64, 768), BF),
            pltpu.VMEM((512, 256), BF),
            pltpu.VMEM((8, 8, 32, 1024), BF),
            pltpu.VMEM((8, 8, 32, 1024), BF),
            pltpu.VMEM((256, 2048), BF),
            pltpu.VMEM((64, 2048), BF),
            pltpu.VMEM((NC1, 8, 2, 32, 1024), BF),
            pltpu.VMEM((NC1, 4, 2, 32, 1024), BF),
            pltpu.VMEM((NC1, 6, 32, 1024), BF),
            pltpu.VMEM((NC1, 6, 32, 1024), BF),
            pltpu.VMEM((NC2, 8, 2, 64, H2), BF),
            pltpu.VMEM((NC2, 4, 2, 64, H2), BF),
            pltpu.VMEM((NC2, 6, 64, H2), BF),
            pltpu.VMEM((NC2, 6, 64, H2), BF),
            pltpu.VMEM((8, 64, 2048), BF),
            pltpu.VMEM((64, 2048), F32),
            pltpu.VMEM((512, 1024), BF),
            pltpu.VMEM((8, 64, 2048), BF),
            dma((20,)), dma((13,)), dma((2, 3)),
            dma((28,)), dma((4,)), dma((18,)), dma((4, 4)),
            dma((NC1, 4)), dma((NC1, 6)), dma((NC2, 4)), dma((NC2, 6)),
            dma((NC1, 7)), dma((NC2, 7)),
        ],
        compiler_params=pltpu.CompilerParams(
            collective_id=0, has_side_effects=True, vmem_limit_bytes=56 * 1024 * 1024
        ),
        name="layer",
    )(
        queries, keys.T, values.T, documents.reshape(4, 1, 128), q_gain.reshape(1, -1),
        k_gain.reshape(1, -1), sink, w_out, resid, n_gain.reshape(1, -1), w_up, w_down.T,
    )
    return out.reshape(rows, width)


def solution(mesh):
    placed = (
        P("sp", None), P("sp", "tp"), P("sp", "tp"), P("sp", "tp"), P("sp"), P(), P(),
        P("tp"), P("tp", None), P(), P("sp", "tp"), P("tp", "sp"),
    )
    return jax.shard_map(
        shards, mesh=mesh, in_specs=placed, out_specs=P("sp", None), check_vma=False
    )
```

```python
import functools

import jax
import jax.numpy as jnp
from jax import lax
from jax.experimental import pallas as pl
from jax.experimental.pallas import tpu as pltpu
from jax.sharding import PartitionSpec as P

EPS = 1e-06
Z, Y, X, C = 8, 8, 4, 2
MESH = pl.DeviceIdType.MESH
BF, F32 = jnp.bfloat16, jnp.float32
NC1, NC2 = 2, 4


def fused(
    q_h, k_h, v_h, doc_h, qg_h, kg_h, sink_h, wout_h, resid_h, gain_h, wup_h, wdt_h, out,
    qg, kg, sink, gain, QX, KX, VX, DX, KN, ATT, WU, WD, WO, RES, PB1, RB1, SND1, RCV1, PB2, RB2, SND2, RCV2, NALL, MID, ACT, ALL,
    loc, left, hr, gr, rr, fr, er, d1r, n1r, d2r, n2r, a1r, a2r,
):
    sp, tp = lax.axis_index("sp"), lax.axis_index("tp")
    z, y = sp // Y, sp % Y
    x, c = tp // C, tp % C
    co = 1 - c

    def at_z(s):
        return (((z + s + Z) % Z) * Y + y, tp)

    def at_y(s):
        return (z * Y + (y + s + Y) % Y, tp)

    def xm(s):
        return (x + s + X) % X

    def at_x(s):
        return (sp, xm(s) * C + c)

    partner = (sp, x * C + co)

    def rc(src, dst, ss, rs, dev):
        return pltpu.make_async_remote_copy(
            src_ref=src, dst_ref=dst, send_sem=ss, recv_sem=rs, device_id=dev, device_id_type=MESH
        )

    def put(src, dst, ss, rs, dev):
        rc(src, dst, ss, rs, dev).start()

    def got(ref, rs):
        rc(ref, ref, left.at[0], rs, partner).wait_recv()

    loads = [
        pltpu.make_async_copy(wup_h, WU.at[z, y], loc.at[0]),
        pltpu.make_async_copy(k_h, KX.at[:, pl.ds(128, 512)], loc.at[1]),
        pltpu.make_async_copy(v_h, VX.at[:, pl.ds(128, 512)], loc.at[2]),
        pltpu.make_async_copy(doc_h, DX.at[pl.ds(1, 4)], loc.at[3]),
        pltpu.make_async_copy(wdt_h, WD.at[z, y], loc.at[4]),
        pltpu.make_async_copy(q_h, QX, loc.at[5]),
        pltpu.make_async_copy(wout_h, WO, loc.at[6]),
        pltpu.make_async_copy(
            resid_h.at[pl.ds(pl.multiple_of(tp * 64, 64), 64)], RES, loc.at[7]
        ),
    ]
    small = [
        pltpu.make_async_copy(src, dst, loc.at[16 + i])
        for i, (src, dst) in enumerate(((qg_h, qg), (kg_h, kg), (sink_h, sink), (gain_h, gain)))
    ]
    for copy in loads[:5] + small + loads[5:]:
        copy.start()
    barrier = pltpu.get_barrier_semaphore()
    after, before = ((sp + 1) % (Z * Y), tp), ((sp + Z * Y - 1) % (Z * Y), tp)
    near = [at_z(1), at_z(-1), at_y(1), at_y(-1), at_x(1), at_x(-1), at_x(2), partner, after, before]
    for dev in near:
        pl.semaphore_signal(barrier, inc=1, device_id=dev, device_id_type=MESH)
    pl.semaphore_wait(barrier, len(near))

    pieces = ((WU, 0, 512, "z"), (WU, 512, 512, "y"))
    ways = ((0, 1), (1, -1))

    def shard_ref(p, e, major, minor, half):
        buf, lo, n, axis = pieces[p]
        zz, yy = ((z + minor + 16) % 8, (y + major + 16) % 8)
        if axis == "y":
            zz, yy = ((z + major + 16) % 8, (y + minor + 16) % 8)
        rows_ = pl.ds(16 * e, 16) if half else slice(None)
        return buf.at[zz, yy, rows_, pl.ds(lo, n)]

    def ring_send(p, d):
        for e, s in ways:
            src = shard_ref(p, e, 0, -s * (d - 1), d == 4)
            dev = at_z(s) if pieces[p][3] == "z" else at_y(s)
            put(src, src, left.at[0], rr.at[d - 1], dev)

    def minor_off(j):
        return jnp.where(j % 2 == 1, -((j + 1) // 2), j // 2)

    def row_copy(p, e, s, d, j, m):
        src = shard_ref(p, e, -s * (d - 1), minor_off(j), False)
        dev = at_y(s) if pieces[p][3] == "z" else at_z(s)
        return rc(src, src, left.at[1], gr.at[m], dev)

    def row_send(p, j):
        for e, s in ways:
            row_copy(p, e, s, 1, j, j).start()

    def ring_step(d):
        got(WU.at[0, 0] if d == 4 else WU.at[0, pl.ds(0, 2)], rr.at[d - 1])
        if d < 4:
            for p in (0, 1):
                ring_send(p, d + 1)
        for j in (2 * d - 1, 2 * d):
            if j < 8:
                for p in (0, 1):
                    row_send(p, j)

    def pump(lo, hi):
        def step(m, _, to):
            d, j = m // 8 + 1, m % 8
            got(WU.at[0, pl.ds(0, 2)], gr.at[m])
            for p in (0, 1):
                for e, s in ways:
                    if to == (0, 1):
                        row_copy(p, e, s, d + 1, j, m + 8).start()
                    elif e in to:
                        row_copy(p, e, s, 4, m - 16, m + 8 - 4 * e).start()
            return 0

        for a, b, to in ((0, 16, (0, 1)), (16, 20, (0,)), (20, 24, (1,)), (24, 28, ())):
            a, b = max(a, lo), min(b, hi)
            if b - a == 1:
                step(a, 0, to)
            elif a < b:
                lax.fori_loop(a, b, functools.partial(step, to=to), 0)

    ring_base = (0, -3, 3, 4)

    def down_ref(e, dz, dy, half):
        ref = WD.at[(z + dz + 16) % 8, (y + dy + 16) % 8]
        return ref.at[pl.ds(16 * e, 16)] if half else ref

    def loop_send(r, d):
        for e, s in ways:
            src = down_ref(e, ring_base[r], -s * (d - 1), d == 4)
            put(src, src, left.at[2], er.at[r, d - 1], at_y(s))

    def loop_step(r, d):
        got(WD.at[0, 0] if d == 4 else WD.at[0, pl.ds(0, 2)], er.at[r, d - 1])
        if d < 4:
            loop_send(r, d + 1)

    def down_copy(e, s, d, j):
        m = 17 if d == 4 else (d - 1) * 8 + j
        src = down_ref(e, -s * (d - 1), minor_off(j), d == 4)
        return rc(src, src, left.at[3], fr.at[m], at_z(s))

    def down_send(d, lo, hi):
        for j in range(lo, hi):
            for e, s in ways:
                down_copy(e, s, d, j).start()

    def down_got(d, j):
        m = 17 if d == 4 else (d - 1) * 8 + j
        got(WD.at[0, 0] if d == 4 else WD.at[0, pl.ds(0, 2)], fr.at[m])

    def chain(d):
        down_got(d, 0)
        if d < 4:
            down_send(d + 1, 0, 1)

    def pass_on(lo, hi):
        def one_row(j, _):
            down_got(1, j)
            for e, s in ways:
                down_copy(e, s, 2, j).start()
            return 0

        lax.fori_loop(lo, hi, one_row, 0)

    def take(lo, hi):
        def one_row(j, _):
            down_got(2, j)
            return 0

        lax.fori_loop(lo, hi, one_row, 0)

    class Exchange:
        def __init__(self, PB, RB, SND, RCV, ds, dr, ns, nr):
            self.PB, self.RB, self.SND, self.RCV = PB, RB, SND, RCV
            self.ds, self.dr, self.ns, self.nr = ds, dr, ns, nr

        def to_partner(self, k):
            for q in (2, 1, 3, 0):
                b = xm(q)
                put(self.PB.at[k, b * C + co], self.RB.at[k, b], self.ds, self.dr.at[k, q],
                    partner)

        def pair(self, k, q, side):
            b = xm(q)
            return self.PB[k, b * C + c, side].astype(F32) + self.RB[k, b, side].astype(F32)

        def partner_got(self, k, q):
            got(self.RB.at[k, xm(q)], self.dr.at[k, q])

        def send(self, k, slot, value, dirn):
            self.SND[k, slot] = value.astype(BF)
            put(self.SND.at[k, slot], self.RCV.at[k, slot], self.ns, self.nr.at[k, slot],
                at_x(dirn))

        def have(self, k, slot):
            got(self.RCV.at[k, slot], self.nr.at[k, slot])
            return self.RCV[k, slot].astype(F32)

        def far(self, k):
            self.partner_got(k, 2)
            straight = self is two and k in direct
            self.send(k, 0, self.pair(k, 2, 0), 2 if straight else 1)
            self.send(k, 1, self.pair(k, 2, 1), 2 if straight else -1)
            self.partner_got(k, 1)
            self.send(k, 2, self.pair(k, 1, 1), 1)
            self.partner_got(k, 3)
            self.send(k, 3, self.pair(k, 3, 0), -1)
            if straight:
                self.send(k, 4, self.pair(k, 1, 0), 1)
                self.send(k, 5, self.pair(k, 3, 1), -1)

        def grow(self, k):
            self.send(k, 4, self.pair(k, 1, 0) + self.have(k, 0), 1)
            self.send(k, 5, self.pair(k, 3, 1) + self.have(k, 1), -1)

        def total(self, k):
            self.partner_got(k, 0)
            left = self.pair(k, 0, 0) + self.have(k, 3) + self.have(k, 4)
            right = self.pair(k, 0, 1) + self.have(k, 2) + self.have(k, 5)
            if self is two and k in direct:
                left, right = left + self.have(k, 0), right + self.have(k, 1)
            return left, right

    class Gather:
        def __init__(self, G, part, mine, s, r, size, direct=()):
            self.G, self.part, self.mine, self.s, self.r = G, part, mine, s, r
            self.size, self.direct = size, direct

        def ref(self, k, q, side, core):
            return self.G.at[(xm(q) * C + core, *self.part(k, side))]

        def go(self, k, slot, q, side, dev):
            ref = self.ref(k, q, side, c)
            src = self.mine.at[self.part(k, side)] if q == 0 else ref
            put(src, ref, self.s, self.r.at[k, min(slot, 6)], dev)

        def wait(self, k, slot, q, side, core):
            got(self.ref(k, q, side, core), self.r.at[k, slot])

        def own(self, k):
            self.go(k, 0, 0, 0, at_x(1))
            self.go(k, 1, 0, 1, at_x(-1))
            self.go(k, 2, 0, 1, at_x(1))
            self.go(k, 3, 0, 0, at_x(-1))
            if k in self.direct:
                self.go(k, 4, 0, 0, at_x(2))
                self.go(k, 5, 0, 1, at_x(2))
            self.go(k, 6, 0, 0, partner)
            self.go(k, 7, 0, 1, partner)

        def forward(self, k):
            self.wait(k, 0, 3, 0, c)
            if k not in self.direct:
                self.go(k, 4, 3, 0, at_x(1))
            self.wait(k, 1, 1, 1, c)
            if k not in self.direct:
                self.go(k, 5, 1, 1, at_x(-1))
            self.go(k, 8, 3, 0, partner)
            self.go(k, 9, 1, 1, partner)

        def forward2(self, k):
            self.wait(k, 2, 3, 1, c)
            self.go(k, 10, 3, 1, partner)
            self.wait(k, 3, 1, 0, c)
            self.go(k, 11, 1, 0, partner)

        def last(self, k):
            self.wait(k, 4, 2, 0, c)
            self.go(k, 12, 2, 0, partner)
            self.wait(k, 5, 2, 1, c)
            self.go(k, 13, 2, 1, partner)

        def finish(self, k):
            got(NALL.at[0] if self.size == 8 else NALL.at[pl.ds(0, 2)], self.r.at[k, 6])

    one = Exchange(PB1, RB1, SND1, RCV1, left.at[4], d1r, left.at[5], n1r)
    two = Exchange(PB2, RB2, SND2, RCV2, left.at[6], d2r, left.at[7], n2r)
    rows = Gather(
        NALL, lambda k, side: (pl.ds(32 * k, 32), pl.ds(side * 1024, 1024)), NALL.at[x * C + c],
        left.at[8], a1r, 16,
    )
    pairs = ((0, -1), (1, -3), (3, 4), (2, -2))

    def block_of(k, side):
        return (z + pairs[k][side] + 8) % 8

    def out_cols(k, side):
        return pl.ds(pl.multiple_of(block_of(k, side) * 256, 256), 256)

    direct = ()
    done = Gather(
        ALL, lambda k, side: (slice(None), out_cols(k, side)), ALL.at[x * C + c], left.at[9], a2r,
        8, direct,
    )

    loads[0].wait()
    ring_send(0, 1)
    ring_send(1, 1)
    for copy in loads[1:4]:
        copy.wait()
    halo = []
    for i, ref in enumerate((KX, VX, DX)):
        part = [
            ref.at[pl.ds(n, 1)] if i == 2 else ref.at[:, pl.ds(128 * n, 128)] for n in range(6)
        ]
        put(part[4], part[0], left.at[10 + i], hr.at[0, i], after)
        put(part[1], part[5], left.at[10 + i], hr.at[1, i], before)
        halo.append((part[0], part[5]))

    row_send(0, 0)
    row_send(1, 0)

    def halo_got(side):
        for i in range(3):
            got(halo[i][side], hr.at[side, i])

    loads[4].wait()
    loop_send(0, 1)
    down_send(1, 0, 1)

    def head_norm(rows_, gain_, ones):
        wide = rows_.astype(F32)
        square = wide * wide
        high = square.astype(BF)
        low = (square - high.astype(F32)).astype(BF)
        mean = (
            jnp.dot(high, ones, preferred_element_type=F32)
            + jnp.dot(low, ones, preferred_element_type=F32)
        ) * (1.0 / 64)
        return (wide * lax.rsqrt(mean + EPS) * gain_).astype(BF)

    def iotas(rows_, cols_):
        return [lax.broadcasted_iota(jnp.int32, (rows_, cols_), i) for i in range(2)]

    for copy in small:
        copy.wait()
    r64, c64 = iotas(64, 64)
    kgain = jnp.sum(jnp.where(r64 == c64, kg[...], 0.0), axis=1, keepdims=True)
    r256, c256 = iotas(256, 256)
    ones256 = (r256 // 64 == c256 // 64).astype(BF)

    def key_norm(lo, n):
        wide = KX[:, lo:lo + n].astype(F32)
        mean = jnp.mean(wide * wide, axis=0, keepdims=True)
        KN[:, lo:lo + n] = (wide * lax.rsqrt(mean + EPS) * kgain).astype(BF)

    key_norm(128, 512)
    loads[5].wait()
    qgain = jnp.concatenate([qg[...]] * 4, axis=1)
    heads = [
        jnp.exp2(jnp.full((1, 1), (tp * 4 + h + 1).astype(F32) * -0.25)) for h in range(4)
    ]
    row = lax.broadcasted_iota(jnp.int32, (128, 128), 0)
    col = lax.broadcasted_iota(jnp.int32, (128, 128), 1)
    span = jnp.abs(
        lax.broadcasted_iota(jnp.int32, (128, 384), 1) - 128
        - lax.broadcasted_iota(jnp.int32, (128, 384), 0)
    ).astype(F32)

    def attend(b):
        qn = head_norm(QX[128 * b:128 * b + 128], qgain, ones256)
        kb, vb = KN[:, 128 * b:128 * b + 384], VX[:, 128 * b:128 * b + 384]
        docs = [DX[b + i].astype(F32) for i in range(3)]
        mine = jnp.transpose(jnp.broadcast_to(docs[1], (128, 128)))
        if b == 0:
            docs[0] = jnp.where(sp == 0, -1.0, docs[0])
        if b == 3:
            docs[2] = jnp.where(sp == Z * Y - 1, -1.0, docs[2])
        allowed = jnp.concatenate(
            [(mine == docs[0]) & (col >= row), mine == docs[1], (mine == docs[2]) & (col <= row)],
            axis=1,
        )
        outs = []
        for h in range(4):
            score = jnp.dot(qn[:, 64 * h:64 * h + 64], kb, preferred_element_type=F32)
            score = score * 0.125 - heads[h] * span
            score = jnp.where(allowed, score, -1e30)
            top = jnp.maximum(jnp.max(score, axis=1, keepdims=True), sink[h])
            p = jnp.exp(score - top)
            denom = jnp.sum(p, axis=1, keepdims=True) + jnp.exp(sink[h] - top)
            mixed = lax.dot_general(
                p.astype(BF), vb, (((1,), (1,)), ((), ())), preferred_element_type=F32
            )
            outs.append((mixed / denom).astype(BF))
        ATT[128 * b:128 * b + 128] = jnp.concatenate(outs, axis=1)

    def project(k):
        a = ATT[...].reshape(8, 2, 32, 256)[:, k].reshape(256, 256)
        p = jnp.dot(a, WO[...], preferred_element_type=F32).astype(BF)
        for side in range(2):
            PB1[k, :, side] = p[:, side * 1024:side * 1024 + 1024].reshape(8, 32, 1024)
        one.to_partner(k)

    def normalise(k):
        lo = 32 * k
        both = one.total(k)
        mid = (RES[lo:lo + 32].astype(F32) + jnp.concatenate(both, axis=1)).astype(BF).astype(F32)
        MID[lo:lo + 32] = mid
        scale = lax.rsqrt(jnp.mean(mid * mid, axis=-1, keepdims=True) + EPS)
        NALL[x * C + c, lo:lo + 32] = (mid * scale * gain[...]).astype(BF)
        rows.own(k)

    def up(n):
        lhs = NALL[...].reshape(512, 2048)
        rhs = WU[:, :, :, n * 512:n * 512 + 512].reshape(2048, 512)
        r = jnp.maximum(jnp.dot(lhs, rhs, preferred_element_type=F32), 0.0)
        ACT[:, n * 512:n * 512 + 512] = (r * r).astype(BF)

    def s_down(k):
        w = jnp.concatenate([WD[block_of(k, side)].reshape(256, 1024) for side in range(2)], axis=0)
        p = lax.dot_general(
            ACT[...], w, (((1,), (1,)), ((), ())), preferred_element_type=F32
        ).astype(BF)
        for side in range(2):
            PB2[k, :, side] = p[:, side * 256:side * 256 + 256].reshape(8, 64, 256)
        two.to_partner(k)

    def s_total(k):
        for side, part in enumerate(two.total(k)):
            cols = out_cols(k, side)
            ALL[x * C + c, :, cols] = (MID[:, cols] + part).astype(BF)
        done.own(k)

    keep = []

    def hand_over(k):
        done.finish(k)
        for side in range(2):
            cols = out_cols(k, side)
            keep.append(
                pltpu.make_async_copy(
                    ALL.at[:, :, cols], out.at[:, :, cols], loc.at[8 + 2 * k + side]
                )
            )
            keep[-1].start()

    def halo_block(side, lo, b):
        halo_got(side)
        key_norm(lo, 128)
        attend(b)

    for f, *args in (
        (attend, 1), (ring_step, 1), (attend, 2), (pump, 0, 1), (halo_block, 0, 0, 0),
        (chain, 1), (ring_step, 2),
        (halo_block, 1, 640, 3), (loop_step, 0, 1), (pump, 1, 3), (loads[6].wait,),
        (loads[7].wait,), (project, 0), (pump, 8, 9), (project, 1), (one.far, 0),
        (one.far, 1), (chain, 2), (ring_step, 3), (pump, 3, 5), (loop_step, 0, 2), (one.grow, 0),
        (pump, 9, 11), (pump, 16, 17), (chain, 3), (ring_step, 4), (one.grow, 1), (pump, 5, 7),
        (pump, 11, 13), (normalise, 0), (loop_step, 0, 3), (normalise, 1), (pump, 17, 18),
        (chain, 4), (pump, 18, 19), (down_send, 1, 1, 2), (pump, 7, 8), (pump, 13, 14),
        (rows.forward, 0), (pump, 14, 15), (pump, 19, 20), (loop_send, 1, 1), (rows.forward2, 0),
        (pump, 20, 21), (loop_step, 0, 4), (down_send, 1, 2, 3), (rows.forward, 1),
        (pump, 15, 16), (pump, 21, 22), (rows.forward2, 1), (pump, 22, 23), (loop_send, 2, 1),
        (rows.last, 0), (down_send, 1, 3, 4), (pump, 24, 25), (loop_send, 3, 1), (rows.last, 1),
        (down_send, 1, 4, 5), (pump, 23, 24), (loop_step, 1, 1), (down_send, 1, 5, 8),
        (pass_on, 1, 3), (pump, 25, 27), (loop_step, 2, 1), (pass_on, 3, 4), (loop_step, 3, 1),
        (pass_on, 4, 5), (pump, 27, 28), (rows.finish, 0), (rows.finish, 1), (up, 0),
        (loop_step, 1, 2), (up, 1), (loop_step, 2, 2), (pass_on, 5, 7), (loop_step, 3, 2),
        (pass_on, 7, 8), (s_down, 0), (loop_step, 1, 3), (take, 1, 2), (two.far, 0),
        (loop_step, 2, 3), (take, 2, 3), (loop_step, 3, 3), (take, 3, 4), (loop_step, 1, 4),
        (s_down, 1), (two.grow, 0), (take, 4, 5), (loop_step, 2, 4), (two.far, 1), (take, 5, 6),
        (loop_step, 3, 4), (s_down, 2), (take, 6, 7), (s_total, 0), (two.far, 2), (take, 7, 8),
        (s_down, 3), (two.grow, 1), (two.far, 3), (done.forward, 0), (done.forward2, 0),
        (two.grow, 2), (s_total, 1), (two.grow, 3), (done.last, 0), (s_total, 2),
        (done.forward, 1), (done.forward2, 1), (s_total, 3), (done.forward, 2),
        (done.forward2, 2), (done.last, 1), (done.forward, 3), (done.forward2, 3),
        (hand_over, 0), (done.last, 2), (hand_over, 1), (done.last, 3), (hand_over, 2),
        (hand_over, 3),
    ):
        f(*args)
    for copy in keep:
        copy.wait()

    for i, ref in enumerate((
        WU.at[0, pl.ds(0, 7)], WU.at[pl.ds(0, 7)], WD.at[pl.ds(0, 7), pl.ds(0, 4)],
        WD.at[pl.ds(0, 7), pl.ds(0, 5)], RB1, SND1, RB2, SND2, NALL.at[pl.ds(0, 7)],
        NALL.at[pl.ds(0, 7)], KX.at[:, pl.ds(0, 256)], VX.at[:, pl.ds(0, 256)],
        DX.at[pl.ds(0, 2)],
    )):
        rc(ref, ref, left.at[i], hr.at[0, 0], partner).wait_send()


def shards(
    resid, queries, keys, values, documents, q_gain, k_gain, sink, w_out, n_gain, w_up, w_down
):
    rows, width = resid.shape
    hbm = pl.BlockSpec(memory_space=pltpu.HBM)
    H2 = 2048 // (2 * NC2)
    dma = pltpu.SemaphoreType.DMA
    out = pl.pallas_call(
        fused,
        out_shape=jax.ShapeDtypeStruct((8, rows // 8, width), BF),
        in_specs=[hbm] * 12,
        out_specs=pl.BlockSpec(memory_space=pl.ANY),
        scratch_shapes=[
            pltpu.VMEM((1, 64), F32),
            pltpu.VMEM((1, 64), F32),
            pltpu.SMEM((4,), F32),
            pltpu.VMEM((1, 2048), F32),
            pltpu.VMEM((512, 256), BF),
            pltpu.VMEM((64, 768), BF),
            pltpu.VMEM((64, 768), BF),
            pltpu.VMEM((6, 1, 128), jnp.int32),
            pltpu.VMEM((64, 768), BF),
            pltpu.VMEM((512, 256), BF),
            pltpu.VMEM((8, 8, 32, 1024), BF),
            pltpu.VMEM((8, 8, 32, 1024), BF),
            pltpu.VMEM((256, 2048), BF),
            pltpu.VMEM((64, 2048), BF),
            pltpu.VMEM((NC1, 8, 2, 32, 1024), BF),
            pltpu.VMEM((NC1, 4, 2, 32, 1024), BF),
            pltpu.VMEM((NC1, 6, 32, 1024), BF),
            pltpu.VMEM((NC1, 6, 32, 1024), BF),
            pltpu.VMEM((NC2, 8, 2, 64, H2), BF),
            pltpu.VMEM((NC2, 4, 2, 64, H2), BF),
            pltpu.VMEM((NC2, 6, 64, H2), BF),
            pltpu.VMEM((NC2, 6, 64, H2), BF),
            pltpu.VMEM((8, 64, 2048), BF),
            pltpu.VMEM((64, 2048), F32),
            pltpu.VMEM((512, 1024), BF),
            pltpu.VMEM((8, 64, 2048), BF),
            dma((20,)), dma((13,)), dma((2, 3)),
            dma((28,)), dma((4,)), dma((18,)), dma((4, 4)),
            dma((NC1, 4)), dma((NC1, 6)), dma((NC2, 4)), dma((NC2, 6)),
            dma((NC1, 7)), dma((NC2, 7)),
        ],
        compiler_params=pltpu.CompilerParams(
            collective_id=0, has_side_effects=True, vmem_limit_bytes=56 * 1024 * 1024
        ),
        name="layer",
    )(
        queries, keys.T, values.T, documents.reshape(4, 1, 128), q_gain.reshape(1, -1),
        k_gain.reshape(1, -1), sink, w_out, resid, n_gain.reshape(1, -1), w_up, w_down.T,
    )
    return out.reshape(rows, width)


def solution(mesh):
    placed = (
        P("sp", None), P("sp", "tp"), P("sp", "tp"), P("sp", "tp"), P("sp"), P(), P(),
        P("tp"), P("tp", None), P(), P("sp", "tp"), P("tp", "sp"),
    )
    return jax.shard_map(
        shards, mesh=mesh, in_specs=placed, out_specs=P("sp", None), check_vma=False
    )
```
